32 devices in a mesh: fs: 8 (over z, y), tp: 4 (over x, core).
Axes of the slice: x: 2, y: 2, z: 4, core: 2. Of those that a mesh axis runs over, the one named last changes fastest.
Arguments:
- mixed: bfloat16 [12288, 2048], P(('fs', 'tp')), may hold values from -6 to 6
- residual: bfloat16 [12288, 2048], P(('fs', 'tp')), may hold values from -6 to 6
- mix_weight: bfloat16 [2048, 2048], P(('fs', 'tp')), may hold values from -0.125 to 0.125
- norm_gain: float32 [2048], replicated, may hold values from 0.1 to 1.9
- up_weight: bfloat16 [2048, 5504], P('fs', 'tp'), may hold values from -0.125 to 0.125
- gate_weight: bfloat16 [2048, 5504], P('fs', 'tp'), may hold values from -0.125 to 0.125
- conv_weight: float32 [3, 5504], P(None, 'tp'), may hold values from -3 to 3
- conv_bias: float32 [5504], P('tp'), may hold values from -3 to 3
- down_weight: bfloat16 [5504, 2048], P('tp', 'fs'), may hold values from -0.078125 to 0.078125
Outputs:
- output: bfloat16 [12288, 2048], P(('fs', 'tp'))
The draws below stay inside these ranges and needn't reach their ends.
All inputs are finite; a program needn't handle non-finite values.
Results may differ from the reference program's by a relative error of at most 0.012.
Values may be sent and summed in bfloat16 or wider, within the bound.
A program may use at most 128 MiB of HBM per device.

```python
import jax
import jax.numpy as jnp
from jax import lax

D = 2048
DM = 2048
FF = 5504
TOK_DEV = 384
TOKENS = 12288
N_FS = 8
N_TP = 4


def block_levels(stream_key, dims, shards, smallest, top_value):
    factor_of = 1.0
    for axis_at, parts in shards:
        steps = jax.random.uniform(jax.random.fold_in(jax.random.fold_in(stream_key, 6), axis_at), (parts,), jnp.float32, smallest / len(shards), top_value / len(shards))
        factor_of = factor_of * jnp.repeat(jnp.exp(steps), dims[axis_at] // parts).reshape((-1,) + (1,) * (len(dims) - 1 - axis_at))
    return factor_of


def scatter_about(own_key, shape, width, bound, pieces=(), kind=jnp.bfloat16):
    loudness = block_levels(own_key, shape, pieces, -0.22, 0.18) if pieces else 1.0
    entries = jax.random.normal(own_key, shape, jnp.float32) * width * loudness
    return jnp.minimum(jnp.maximum(entries, -bound), bound).astype(kind)


def setup_inputs(seed: int = 0) -> dict:
    streams_of = jax.random.split(jax.random.key(seed), 10)
    return {
        "mixed": scatter_about(streams_of[0], (TOKENS, DM), 1.0, 6.0, ((0, 32),)),
        "residual": scatter_about(streams_of[1], (TOKENS, D), 1.0, 6.0, ((0, 32),)),
        "mix_weight": scatter_about(streams_of[2], (DM, D), DM ** -0.5, 0.125, ((0, 32),)),
        "norm_gain": jnp.clip(1.0 + 0.18 * jax.random.normal(streams_of[3], (D,), jnp.float32), 0.1, 1.9),
        "up_weight": scatter_about(streams_of[4], (D, FF), D ** -0.5, 0.125, ((0, 8), (1, 4))),
        "gate_weight": scatter_about(streams_of[5], (D, FF), D ** -0.5, 0.125, ((0, 8), (1, 4))),
        "conv_weight": scatter_about(streams_of[6], (3, FF), 0.577, 3.0, ((1, 4),), jnp.float32),
        "conv_bias": scatter_about(streams_of[7], (FF,), 0.5, 3.0, ((0, 4),), jnp.float32),
        "down_weight": scatter_about(streams_of[8], (FF, D), FF ** -0.5, 0.078125, ((0, 4), (1, 8))),
    }


norm_eps = 1e-06

def reference(mixed, residual, mix_weight, norm_gain, up_weight, gate_weight, conv_weight, conv_bias, down_weight):
    unit_block = FF // N_TP
    length = TOK_DEV * N_TP
    stream = (residual.astype(jnp.float32) + jnp.dot(mixed, mix_weight, preferred_element_type=jnp.float32)).astype(jnp.bfloat16)
    x_float = stream.astype(jnp.float32)
    normed = (x_float * lax.rsqrt(lax.optimization_barrier(jnp.mean(x_float * x_float, axis=-1, keepdims=True)) + norm_eps) * norm_gain).astype(jnp.bfloat16)

    def one_seq(pair):
        normed_seq, stream_seq = pair
        up_part = jnp.dot(normed_seq, up_weight, preferred_element_type=jnp.float32).astype(jnp.bfloat16)
        gate_part = jnp.dot(normed_seq, gate_weight, preferred_element_type=jnp.float32).astype(jnp.bfloat16)
        up_float = lax.optimization_barrier(up_part).astype(jnp.float32)
        padded = jnp.pad(up_float, ((2, 0), (0, 0)))
        smoothed = conv_bias + conv_weight[0] * padded[:-2] + conv_weight[1] * padded[1:-1] + conv_weight[2] * padded[2:]
        hidden = (jax.nn.gelu(smoothed) * gate_part.astype(jnp.float32)).astype(jnp.bfloat16)
        accum_sum = stream_seq.astype(jnp.float32)
        for index in range(N_TP):
            partial_value = jnp.dot(hidden[:, index * unit_block:(index + 1) * unit_block], down_weight[index * unit_block:(index + 1) * unit_block], preferred_element_type=jnp.float32).astype(jnp.bfloat16)
            accum_sum = accum_sum + lax.optimization_barrier(partial_value).astype(jnp.float32)
        return accum_sum.astype(jnp.bfloat16)
    result = lax.map(one_seq, (normed.reshape(N_FS, length, D), stream.reshape(N_FS, length, D)))
    return result.reshape(N_FS * length, D)
```

```python
import functools

import jax
import jax.numpy as jnp
from jax import lax
from jax.experimental import pallas as pl
from jax.experimental.pallas import tpu as pltpu
from jax.sharding import PartitionSpec as P

norm_eps = 1e-06
f32, bf16 = jnp.float32, jnp.bfloat16
MESH = pl.DeviceIdType.MESH
NT = (((1,), (1,)), ((), ()))
TILE = 256


def mod(a, n):
    return lax.rem(a + n, n)


def ring_place(f, nz, ny):
    z, y = lax.div(f, ny), lax.rem(f, ny)
    if ny == 1:
        return z
    along = jnp.where(lax.rem(z, 2) == 0, y - 1, ny - 1 - y)
    return jnp.where(y == 0, nz * (ny - 1) + nz - 1 - z, z * (ny - 1) + along)


def ring_chip(r, nz, ny):
    if ny == 1:
        return r
    z, k = lax.div(r, ny - 1), lax.rem(r, ny - 1)
    out = z * ny + jnp.where(lax.rem(z, 2) == 0, 1 + k, ny - 1 - k)
    return jnp.where(r < nz * (ny - 1), out, (nz - 1 - (r - nz * (ny - 1))) * ny)


def layer_kernel(
    nz,
    ny,
    nx,
    mixed,
    residual,
    mix_shard,
    up_shard,
    gate_shard,
    down_shard,
    gain,
    taps,
    bias,
    out,
    mix_full,
    up_full,
    gate_full,
    down_full,
    tokens,
    up_part,
    hidden,
    mixed_v,
    held,
    stream,
    keep,
    got_core,
    got_x,
    w_send,
    w_recv,
    mr_send,
    m_recv,
    mx_send,
    mc_send,
    t_recv,
    tx_send,
    tc_send,
    pc_send,
    pc_recv,
    px_send,
    px_recv,
    in_sem,
    out_sem,
):
    n = nz * ny
    half_n = n // 2
    n_tp = 2 * nx
    me = lax.axis_index("fs")
    tp = lax.axis_index("tp")
    x, core = lax.div(tp, 2), lax.rem(tp, 2)
    place = ring_place(me, nz, ny)

    def ring(d):
        return ring_chip(mod(place + d, n), nz, ny)

    nxt, prv = ring(1), ring(-1)
    twin = tp + 1 - 2 * core

    def x_at(dx):
        return lax.rem(x + dx, nx) * 2 + core

    tok, width = stream.shape
    hid, wide = up_shard.shape
    cut = (hid // 2 + 15) // 16 * 16
    halves = ((0, cut), (cut, hid - cut))
    fulls = (up_full, gate_full, down_full)
    shards = (up_shard, gate_shard, down_shard)
    n_step = n - 3
    mrows = mix_shard.shape[0]

    def remote(src, dst, send, recv, axis, to):
        return pltpu.make_async_remote_copy(
            src_ref=src,
            dst_ref=dst,
            send_sem=send,
            recv_sem=recv,
            device_id={axis: to},
            device_id_type=MESH,
        )

    def slot(m, f, h):
        off, size = halves[h]
        return fulls[m].at[pl.ds(off, size), pl.ds(pl.multiple_of(f * wide, 128), wide)]

    def w_copy(m, f, h, way, mine=False):
        off, size = halves[h]
        src = shards[m].at[pl.ds(off, size), :] if mine else slot(m, f, h)
        to = prv if way else nxt
        return remote(src, slot(m, f, h), w_send.at[m, way, f, h], w_recv.at[m, f, h], "fs", to)

    def w_own(m):
        for k in range(2):
            w_copy(m, me, k, 0, True).start()
            w_copy(m, me, 1 - k, 1, True).start()

    def w_step(m, k):
        d, h = 1 + k // 2, k % 2
        for way, f, hh in ((0, ring(-d), h), (1, ring(d), 1 - h)):
            w_copy(m, f, hh, way).wait_recv()
            if k < n_step:
                w_copy(m, f, hh, way).start()

    def w_drain(m):
        for h in range(2):
            for way in range(2):
                w_copy(m, me, h, way, True).wait_send()
        for k in range(n_step):
            d, h = 1 + k // 2, k % 2
            w_copy(m, ring(-d), h, 0).wait_send()
            w_copy(m, ring(d), 1 - h, 1).wait_send()

    def w_local(m):
        cols = pl.ds(pl.multiple_of(me * wide, 128), wide)
        return pltpu.make_async_copy(shards[m], fulls[m].at[:, cols], in_sem.at[m])

    def part(f, t):
        return mix_full.at[pl.ds(pl.multiple_of((f * n_tp + t) * mrows, 16), mrows), :]

    def m_ring(f, way, mine=False):
        src = mix_shard if mine else part(f, tp)
        to = prv if way else nxt
        return remote(src, part(f, tp), mr_send.at[way, f], m_recv.at[f, tp], "fs", to)

    def m_x(f, dx, mine=False):
        src = mix_shard if mine else part(f, tp)
        return remote(src, part(f, tp), mx_send.at[f, dx - 1], m_recv.at[f, tp], "tp", x_at(dx))

    def m_core(f, dx, mine=False):
        t = x_at(dx)
        src = mix_shard if mine else part(f, t)
        return remote(src, part(f, t), mc_send.at[f, dx], m_recv.at[f, t], "tp", twin)

    def m_spread(f, mine=False):
        for dx in range(1, nx):
            m_x(f, dx, mine).start()
        m_core(f, 0, mine).start()

    def m_wait(f, t):
        remote(part(f, t), part(f, t), mc_send.at[f, 0], m_recv.at[f, t], "tp", twin).wait_recv()

    def m_step(d):
        for way in range(2):
            if d < half_n + 1 - way:
                f = ring(d if way else -d)
                m_wait(f, tp)
                if d < half_n - way:
                    m_ring(f, way).start()
                m_spread(f)

    def m_relay(f):
        for dx in range(1, nx):
            m_wait(f, x_at(dx))
            m_core(f, dx).start()

    def m_drain():
        for q in range(n):
            d = (q + 1) // 2
            f = ring(-d if q % 2 else d)
            mine = q == 0
            for way in range(2):
                if d < half_n - way and (mine or (q % 2 == 1) == (way == 0)):
                    m_ring(f, way, mine).wait_send()
            for dx in range(1, nx):
                m_x(f, dx, mine).wait_send()
            for dx in range(nx):
                m_core(f, dx, mine and dx == 0).wait_send()

    def rows(b):
        return pl.ds(pl.multiple_of(b * tok, 16), tok)

    def t_copy(b, send, to):
        return remote(tokens.at[rows(b), :], tokens.at[rows(b), :], send, t_recv.at[b], "tp", to)

    def t_wait(b):
        t_copy(b, tc_send.at[0], twin).wait_recv()

    def columns(f):
        return pl.ds(pl.multiple_of(f * wide, 128), wide)

    def gone(dx, q):
        return mix_full.at[pl.ds(dx * tok, tok), columns(q)]

    def pc_copy(dx, q):
        return remote(
            gone(dx, q), got_core.at[dx, q], pc_send.at[q, dx], pc_recv.at[q, dx], "tp", twin
        )

    def px_copy(dx, q):
        return remote(
            keep.at[dx, q],
            got_x.at[dx - 1, q],
            px_send.at[q, dx - 1],
            px_recv.at[q, dx - 1],
            "tp",
            x_at(dx),
        )

    def out_copy(f, q):
        return pltpu.make_async_copy(held.at[:, columns(f)], out.at[:, columns(f)], out_sem.at[q])

    load_mixed = pltpu.make_async_copy(mixed, mixed_v, in_sem.at[3])
    load_residual = pltpu.make_async_copy(residual, held, in_sem.at[4])
    load_mix = pltpu.make_async_copy(mix_shard, part(me, tp), in_sem.at[5])

    barrier = pltpu.get_barrier_semaphore()
    for other in (nxt, prv):
        pl.semaphore_signal(barrier, inc=1, device_id={"fs": other}, device_id_type=MESH)
    for other in [twin] + [x_at(dx) for dx in range(1, nx)]:
        pl.semaphore_signal(barrier, inc=1, device_id={"tp": other}, device_id_type=MESH)
    pl.semaphore_wait(barrier, 2 + nx)

    m_ring(me, 0, True).start()
    m_ring(me, 1, True).start()
    m_spread(me, True)
    load_mix.start()
    load_mixed.start()
    load_residual.start()
    w_own(0)
    for m in range(3):
        w_local(m).start()
    up_part[0:16, :] = jnp.zeros((16, hid), bf16)

    early = min(n_step, half_n - 1)
    for d in range(1, half_n + 1):
        m_step(d)
        if 2 <= d < early + 2:
            w_step(0, d - 2)
    for q in range(n):
        d = (q + 1) // 2
        m_relay(ring(-d if q % 2 else d))
    for f in range(n):
        for dx in range(nx):
            m_wait(f, x_at(dx) + 1 - 2 * core)
    load_mix.wait()
    load_mixed.wait()
    load_residual.wait()

    def project(i, _):
        cols = pl.ds(pl.multiple_of(i * TILE, 128), TILE)
        made = jnp.dot(mixed_v[...], mix_full[:, cols], preferred_element_type=f32)
        stream[:, cols] = (held[:, cols].astype(f32) + made).astype(bf16)
        return 0

    lax.fori_loop(0, width // TILE, project, 0)

    for k in range(early, min(early + 1, n_step)):
        w_step(0, k)

    def norm(i, _):
        at = pl.multiple_of(i * 32, 16)
        row = stream[pl.ds(at, 32), :].astype(f32)
        scale = lax.rsqrt(jnp.mean(row * row, axis=-1, keepdims=True) + norm_eps)
        tokens[pl.ds(pl.multiple_of(tp * tok + at, 16), 32), :] = (row * scale * gain[...]).astype(
            bf16
        )
        return 0

    lax.fori_loop(0, tok // 32, norm, 0)
    for dx in range(1, nx):
        t_copy(tp, tx_send.at[dx - 1], x_at(dx)).start()
    t_copy(tp, tc_send.at[0], twin).start()

    for k in range(min(early + 1, n_step), n_step):
        w_step(0, k)
    w_own(1)
    for k in range(n_step, n - 1):
        w_step(0, k)
    w_local(0).wait()

    def block_of(j):
        return lax.rem(x + lax.div(j, 2), nx) * 2 + lax.rem(core + lax.rem(j, 2), 2)

    def up_block(j, _):
        b = block_of(j)

        @pl.when(j > 0)
        def _():
            t_wait(b)

        @pl.when((j > 1) & (lax.rem(j, 2) == 0))
        def _():
            t_copy(b, tc_send.at[lax.div(j, 2)], twin).start()

        for lo in range(0, hid, TILE):
            hi = min(lo + TILE, hid)
            made = lax.dot_general(
                tokens[rows(b), :], up_full[lo:hi, :], NT, preferred_element_type=f32
            )
            up_part[pl.ds(pl.multiple_of(16 + b * tok, 16), tok), lo:hi] = made.astype(bf16)
        for k in range(n_step):

            @pl.when(j == min(n_tp - 1, ((k + 1) * n_tp - 1) // n_step))
            def _():
                w_step(1, k)

        return 0

    lax.fori_loop(0, n_tp, up_block, 0)
    w_own(2)
    for k in range(n_step, n - 1):
        w_step(1, k)
    w_local(1).wait()
    m_drain()

    def gate_block(j, _):
        b = block_of(j)
        for lo in range(0, hid, TILE):
            hi = min(lo + TILE, hid)
            made = lax.dot_general(
                tokens[rows(b), :], gate_full[lo:hi, :], NT, preferred_element_type=f32
            )
            gated = made.astype(bf16).astype(f32)
            window = up_part[pl.ds(pl.multiple_of(b * tok, 16), tok + 16), lo:hi].astype(f32)
            smoothed = bias[:, lo:hi]
            for k in range(3):
                moved = window if k == 2 else pltpu.roll(window, 2 - k, 0)
                smoothed = smoothed + taps[k : k + 1, lo:hi] * moved[16:, :]
            hidden[rows(b), lo:hi] = (jax.nn.gelu(smoothed) * gated).astype(bf16)
        for k in range(min(n_tp - 1, n_step)):

            @pl.when(j == k + 1)
            def _():
                w_step(2, k)

        return 0

    lax.fori_loop(0, n_tp, gate_block, 0)
    w_local(2).wait()

    def shard_of(q):
        d = lax.div(q + 1, 2)
        return ring(jnp.where(lax.rem(q, 2) == 1, -d, d))

    def down_step(q, _):
        for d in range(1, half_n + 1):
            late = [k for k in (2 * d - 2, 2 * d - 1) if min(n_tp - 1, n_step) <= k <= n - 2]
            if late:

                @pl.when(q == 2 * d - 1)
                def _():
                    for k in late:
                        w_step(2, k)

        @pl.when(q < n)
        def _():
            weight = down_full[:, columns(shard_of(q))]
            for dx in range(nx):
                b = x_at(dx) + 1 - 2 * core
                made = jnp.dot(hidden[rows(b), :], weight, preferred_element_type=f32)
                gone(dx, q)[...] = made.astype(bf16)
            for dx in range(nx):
                made = jnp.dot(hidden[rows(x_at(dx)), :], weight, preferred_element_type=f32)
                keep[dx, q] = made.astype(bf16)
                pc_copy(dx, q).start()

        @pl.when((q > 0) & (q < n + 1))
        def _():
            p = q - 1
            for dx in list(range(1, nx)) + [0]:
                pc_copy(dx, p).wait_recv()
                if dx:
                    both = keep[dx, p].astype(f32) + got_core[dx, p].astype(f32)
                    keep[dx, p] = both.astype(bf16)
                    px_copy(dx, p).start()

        @pl.when(q > 1)
        def _():
            p = q - 2
            f = shard_of(p)
            total = stream[:, columns(f)].astype(f32)
            total = total + keep[0, p].astype(f32) + got_core[0, p].astype(f32)
            for dx in range(1, nx):
                px_copy(dx, p).wait_recv()
                total = total + got_x[dx - 1, p].astype(f32)
            held[:, columns(f)] = total.astype(bf16)
            out_copy(f, p).start()

        return 0

    lax.fori_loop(0, n + 2, down_step, 0)

    def finish(q, _):
        out_copy(shard_of(q), q).wait()
        for dx in range(nx):
            pc_copy(dx, q).wait_send()
            if dx:
                px_copy(dx, q).wait_send()
        return 0

    lax.fori_loop(0, n, finish, 0)
    for dx in range(1, nx):
        t_copy(tp, tx_send.at[dx - 1], x_at(dx)).wait_send()
    for dx in range(nx):
        t_copy(x_at(dx), tc_send.at[dx], twin).wait_send()
    for m in range(3):
        w_drain(m)


def make_body(n_fs, n_tp, ny):
    nz, nx = n_fs // ny, n_tp // 2

    def body(
        mixed,
        residual,
        mix_weight,
        norm_gain,
        up_weight,
        gate_weight,
        conv_weight,
        conv_bias,
        down_weight,
    ):
        tok, width = residual.shape
        depth, (hid, wide) = mixed.shape[1], down_weight.shape
        dma = pltpu.SemaphoreType.DMA
        whole = pl.BlockSpec(memory_space=pl.ANY)
        small = pl.BlockSpec(memory_space=pltpu.VMEM)
        return pl.pallas_call(
            functools.partial(layer_kernel, nz, ny, nx),
            out_shape=jax.ShapeDtypeStruct((tok, width), bf16),
            in_specs=[whole] * 6 + [small] * 3,
            out_specs=whole,
            scratch_shapes=[
                pltpu.VMEM((depth, width), bf16),
                pltpu.VMEM((hid, width), bf16),
                pltpu.VMEM((hid, width), bf16),
                pltpu.VMEM((hid, width), bf16),
                pltpu.VMEM((n_tp * tok, width), bf16),
                pltpu.VMEM((n_tp * tok + 16, hid), bf16),
                pltpu.VMEM((n_tp * tok, hid), bf16),
                pltpu.VMEM((tok, depth), bf16),
                pltpu.VMEM((tok, width), bf16),
                pltpu.VMEM((tok, width), bf16),
                pltpu.VMEM((nx, n_fs, tok, wide), bf16),
                pltpu.VMEM((nx, n_fs, tok, wide), bf16),
                pltpu.VMEM((max(nx - 1, 1), n_fs, tok, wide), bf16),
                dma((3, 2, n_fs, 2)),
                dma((3, n_fs, 2)),
                dma((2, n_fs)),
                dma((n_fs, n_tp)),
                dma((n_fs, max(nx - 1, 1))),
                dma((n_fs, nx)),
                dma((n_tp,)),
                dma((max(nx - 1, 1),)),
                dma((nx,)),
                dma((n_fs, nx)),
                dma((n_fs, nx)),
                dma((n_fs, max(nx - 1, 1))),
                dma((n_fs, max(nx - 1, 1))),
                dma((6,)),
                dma((n_fs,)),
            ],
            compiler_params=pltpu.CompilerParams(
                collective_id=0, has_side_effects=True, vmem_limit_bytes=67043328
            ),
        )(
            mixed,
            residual,
            mix_weight,
            up_weight.T,
            gate_weight.T,
            down_weight,
            norm_gain[None, :],
            conv_weight,
            conv_bias[None, :],
        )

    return body


def solution(mesh):
    coords = [getattr(d, "coords", None) for d in mesh.devices[:, 0]]
    n_fs, n_tp = mesh.shape["fs"], mesh.shape["tp"]
    ny = len({c[1] for c in coords}) if None not in coords else 1
    if n_fs % ny:
        ny = 1
    return jax.shard_map(
        make_body(n_fs, n_tp, ny),
        mesh=mesh,
        in_specs=(
            P(("fs", "tp"), None),
            P(("fs", "tp"), None),
            P(("fs", "tp"), None),
            P(),
            P("fs", "tp"),
            P("fs", "tp"),
            P(None, "tp"),
            P("tp"),
            P("tp", "fs"),
        ),
        out_specs=P(("fs", "tp"), None),
        check_vma=False,
    )
```

```python
import functools

import jax
import jax.numpy as jnp
from jax import lax
from jax.experimental import pallas as pl
from jax.experimental.pallas import tpu as pltpu
from jax.sharding import PartitionSpec as P

norm_eps = 1e-06
f32, bf16 = jnp.float32, jnp.bfloat16
MESH = pl.DeviceIdType.MESH
NT = (((1,), (1,)), ((), ()))
TILE = 256
VMEM = 67043328


def mod(a, n):
    return lax.rem(a + n, n)


def ring_place(f, nz, ny):
    z, y = lax.div(f, ny), lax.rem(f, ny)
    if ny == 1:
        return z
    along = jnp.where(lax.rem(z, 2) == 0, y - 1, ny - 1 - y)
    return jnp.where(y == 0, nz * (ny - 1) + nz - 1 - z, z * (ny - 1) + along)


def ring_chip(r, nz, ny):
    if ny == 1:
        return r
    z, k = lax.div(r, ny - 1), lax.rem(r, ny - 1)
    out = z * ny + jnp.where(lax.rem(z, 2) == 0, 1 + k, ny - 1 - k)
    return jnp.where(r < nz * (ny - 1), out, (nz - 1 - (r - nz * (ny - 1))) * ny)


def layer_kernel(
    nz,
    ny,
    nx,
    split,
    mixed,
    residual,
    mix_shard,
    up_shard,
    gate_shard,
    down_shard,
    gain,
    taps,
    bias,
    out,
    mix_full,
    up_full,
    gate_full,
    down_full,
    tokens,
    up_part,
    hidden,
    gate_sum,
    mixed_v,
    held,
    stream,
    keep,
    got_core,
    got_x,
    w_send,
    w_recv,
    mr_send,
    m_recv,
    end_recv,
    mx_send,
    mc_send,
    t_recv,
    tx_send,
    tc_send,
    pc_send,
    pc_recv,
    px_send,
    px_recv,
    in_sem,
    out_sem,
):
    n = nz * ny
    half_n = n // 2
    n_tp = 2 * nx
    me = lax.axis_index("fs")
    tp = lax.axis_index("tp")
    x, core = lax.div(tp, 2), lax.rem(tp, 2)
    place = ring_place(me, nz, ny)

    chips = [ring_chip(mod(place + d, n), nz, ny) for d in range(n)]

    def ring(d):
        return chips[d % n]

    nxt, prv = ring(1), ring(-1)
    twin = tp + 1 - 2 * core

    def x_at(dx):
        return lax.rem(x + dx, nx) * 2 + core

    tok, width = stream.shape
    hid, wide = up_shard.shape
    cut = (hid // 2 + 15) // 16 * 16
    halves = ((0, cut), (cut, hid - cut))
    fulls = (up_full, gate_full, down_full)
    shards = (up_shard, gate_shard, down_shard)
    n_step = n - 3
    mrows = mix_shard.shape[0]

    def remote(src, dst, send, recv, axis, to):
        return pltpu.make_async_remote_copy(
            src_ref=src,
            dst_ref=dst,
            send_sem=send,
            recv_sem=recv,
            device_id={axis: to},
            device_id_type=MESH,
        )

    def slot(m, f, h):
        off, size = halves[h]
        return fulls[m].at[pl.ds(off, size), pl.ds(pl.multiple_of(f * wide, 128), wide)]

    def w_copy(m, f, h, way, mine=False):
        off, size = halves[h]
        src = shards[m].at[pl.ds(off, size), :] if mine else slot(m, f, h)
        to = prv if way else nxt
        return remote(src, slot(m, f, h), w_send.at[m, way, f, h], w_recv.at[m, f, h], "fs", to)

    def w_own(m):
        for k in range(2):
            w_copy(m, me, k, 0, True).start()
            w_copy(m, me, 1 - k, 1, True).start()

    def w_step(m, k):
        d, h = 1 + k // 2, k % 2
        for way, f, hh in ((0, ring(-d), h), (1, ring(d), 1 - h)):
            w_copy(m, f, hh, way).wait_recv()
            if k < n_step:
                w_copy(m, f, hh, way).start()

    def w_drain(m):
        for h in range(2):
            for way in range(2):
                w_copy(m, me, h, way, True).wait_send()
        for k in range(n_step):
            d, h = 1 + k // 2, k % 2
            w_copy(m, ring(-d), h, 0).wait_send()
            w_copy(m, ring(d), 1 - h, 1).wait_send()

    def w_local(m):
        cols = pl.ds(pl.multiple_of(me * wide, 128), wide)
        return pltpu.make_async_copy(shards[m], fulls[m].at[:, cols], in_sem.at[m])

    def part(f, t):
        return mix_full.at[pl.ds(pl.multiple_of((f * n_tp + t) * mrows, 16), mrows), :]

    def m_ring(f, way, mine=False, last=False):
        src, dst = mix_shard if mine else part(f, tp), part(f, tp)
        to, got = prv if way else nxt, m_recv.at[f, tp]
        if last:
            cols = pl.ds(way * (width // 2), width // 2)
            src = dst = dst.at[:, cols]
            got = end_recv.at[way]
        return remote(src, dst, mr_send.at[way, f], got, "fs", to)

    def m_x(f, dx, mine=False):
        src = mix_shard if mine else part(f, tp)
        return remote(src, part(f, tp), mx_send.at[f, dx - 1], m_recv.at[f, tp], "tp", x_at(dx))

    def m_core(f, dx, mine=False):
        t = x_at(dx)
        src = mix_shard if mine else part(f, t)
        return remote(src, part(f, t), mc_send.at[f, dx], m_recv.at[f, t], "tp", twin)

    def m_spread(f, mine=False):
        for dx in range(1, nx):
            m_x(f, dx, mine).start()
        m_core(f, 0, mine).start()

    def m_wait(f, t):
        remote(part(f, t), part(f, t), mc_send.at[f, 0], m_recv.at[f, t], "tp", twin).wait_recv()

    def m_step(d):
        if d == half_n:
            for way in range(2):
                m_ring(ring(d), way, last=True).wait_recv()
            m_spread(ring(d))
            return
        for way in range(2):
            f = ring(d if way else -d)
            m_wait(f, tp)
            m_ring(f, way, last=d == half_n - 1).start()
            m_spread(f)

    def m_relay(f):
        for dx in range(1, nx):
            m_wait(f, x_at(dx))
            m_core(f, dx).start()

    def m_drain():
        for q in range(n):
            d = (q + 1) // 2
            f = ring(-d if q % 2 else d)
            mine = q == 0
            for way in range(2):
                if d < half_n and (mine or (q % 2 == 1) == (way == 0)):
                    m_ring(f, way, mine, d == half_n - 1).wait_send()
            for dx in range(1, nx):
                m_x(f, dx, mine).wait_send()
            for dx in range(nx):
                m_core(f, dx, mine and dx == 0).wait_send()

    def rows(b):
        return pl.ds(pl.multiple_of(b * tok, 16), tok)

    def t_copy(b, send, to):
        return remote(tokens.at[rows(b), :], tokens.at[rows(b), :], send, t_recv.at[b], "tp", to)

    def t_wait(b):
        t_copy(b, tc_send.at[0], twin).wait_recv()

    def columns(f):
        return pl.ds(pl.multiple_of(f * wide, 128), wide)

    def gone(dx, q):
        return mix_full.at[pl.ds(dx * tok, tok), columns(q)]

    def pc_copy(dx, q):
        return remote(
            gone(dx, q), got_core.at[dx, q], pc_send.at[q, dx], pc_recv.at[q, dx], "tp", twin
        )

    def px_copy(dx, q):
        return remote(
            keep.at[dx, q],
            got_x.at[dx - 1, q],
            px_send.at[q, dx - 1],
            px_recv.at[q, dx - 1],
            "tp",
            x_at(dx),
        )

    def out_copy(f, q):
        return pltpu.make_async_copy(held.at[:, columns(f)], out.at[:, columns(f)], out_sem.at[q])

    load_mixed = pltpu.make_async_copy(mixed, mixed_v, in_sem.at[3])
    load_residual = pltpu.make_async_copy(residual, held, in_sem.at[4])
    load_mix = pltpu.make_async_copy(mix_shard, part(me, tp), in_sem.at[5])

    barrier = pltpu.get_barrier_semaphore()
    for other in (nxt, prv):
        pl.semaphore_signal(barrier, inc=1, device_id={"fs": other}, device_id_type=MESH)
    for other in [twin] + [x_at(dx) for dx in range(1, nx)]:
        pl.semaphore_signal(barrier, inc=1, device_id={"tp": other}, device_id_type=MESH)
    pl.semaphore_wait(barrier, 2 + nx)

    m_ring(me, 0, True).start()
    m_ring(me, 1, True).start()
    m_spread(me, True)
    load_mix.start()
    load_mixed.start()
    load_residual.start()
    for m in range(3):
        w_local(m).start()
    up_part[0:16, :] = jnp.zeros((16, hid), bf16)

    early = min(n_step, half_n - 1)
    for d in range(1, half_n + 1):
        m_step(d)
        if d == 1:
            w_own(0)
        if 2 <= d < early + 2:
            w_step(0, d - 2)
    for q in range(n):
        d = (q + 1) // 2
        m_relay(ring(-d if q % 2 else d))
    for f in range(n):
        for dx in range(nx):
            m_wait(f, x_at(dx) + 1 - 2 * core)
    load_mix.wait()
    load_mixed.wait()
    load_residual.wait()

    def project(i, _):
        cols = pl.ds(pl.multiple_of(i * TILE, 128), TILE)
        made = jnp.dot(mixed_v[...], mix_full[:, cols], preferred_element_type=f32)
        stream[:, cols] = (held[:, cols].astype(f32) + made).astype(bf16)
        return 0

    lax.fori_loop(0, width // TILE, project, 0)

    for k in range(early, min(early + 1, n_step)):
        w_step(0, k)

    def norm(i, _):
        at = pl.multiple_of(i * 32, 16)
        row = stream[pl.ds(at, 32), :].astype(f32)
        scale = lax.rsqrt(jnp.mean(row * row, axis=-1, keepdims=True) + norm_eps)
        tokens[pl.ds(pl.multiple_of(tp * tok + at, 16), 32), :] = (row * scale * gain[...]).astype(
            bf16
        )
        return 0

    lax.fori_loop(0, tok // 32, norm, 0)
    for dx in range(1, nx):
        t_copy(tp, tx_send.at[dx - 1], x_at(dx)).start()
    t_copy(tp, tc_send.at[0], twin).start()

    for k in range(min(early + 1, n_step), n_step):
        w_step(0, k)
    w_own(1)
    for k in range(n_step, n - 1):
        w_step(0, k)
    w_local(0).wait()

    def block_of(j):
        return lax.rem(x + lax.div(j, 2), nx) * 2 + lax.rem(core + lax.rem(j, 2), 2)

    def up_block(j, _):
        b = block_of(j)

        @pl.when(j > 0)
        def _():
            t_wait(b)

        @pl.when((j > 1) & (lax.rem(j, 2) == 0))
        def _():
            t_copy(b, tc_send.at[lax.div(j, 2)], twin).start()

        for lo in range(0, hid, TILE):
            hi = min(lo + TILE, hid)
            made = lax.dot_general(
                tokens[rows(b), :], up_full[lo:hi, :], NT, preferred_element_type=f32
            )
            up_part[pl.ds(pl.multiple_of(16 + b * tok, 16), tok), lo:hi] = made.astype(bf16)
        for at, ks in ((1, (0, 1)), (n_tp - 2, (2,))):
            for k in ks:
                if k < ahead:

                    @pl.when(j == at)
                    def _():
                        w_step(1, k)

        return 0

    ahead = min(3, n_step)
    lax.fori_loop(0, n_tp, up_block, 0)

    def gate_dot(b, lo, hi, fs):
        made = None
        for f in fs:
            term = lax.dot_general(
                tokens[rows(b), columns(f)],
                gate_full[lo:hi, columns(f)],
                NT,
                preferred_element_type=f32,
            )
            made = term if made is None else made + term
        return made

    def gate_pass(d):
        fs = ([me] if d == 1 else []) + [ring(-d), ring(d)]

        def add(b, _):
            for lo in range(0, hid, TILE):
                hi = min(lo + TILE, hid)
                made = gate_dot(b, lo, hi, fs)
                if d > 1:
                    made = gate_sum[rows(b), lo:hi] + made
                gate_sum[rows(b), lo:hi] = made
            return 0

        lax.fori_loop(0, n_tp, add, 0)

    w_local(1).wait()
    for d in range(1, half_n):
        for k in (2 * d - 2, 2 * d - 1):
            if k >= ahead:
                w_step(1, k)
            if k == n_step - 1:
                w_own(2)
        if split:
            gate_pass(d)
    w_step(1, n - 2)
    m_drain()

    def gate_block(j, _):
        b = block_of(j)
        for lo in range(0, hid, TILE):
            hi = min(lo + TILE, hid)
            if split:
                made = gate_sum[rows(b), lo:hi] + gate_dot(b, lo, hi, [ring(half_n)])
            else:
                made = lax.dot_general(
                    tokens[rows(b), :], gate_full[lo:hi, :], NT, preferred_element_type=f32
                )
            gated = made.astype(bf16).astype(f32)
            window = up_part[pl.ds(pl.multiple_of(b * tok, 16), tok + 16), lo:hi].astype(f32)
            smoothed = bias[lo:hi][None, :]
            for k in range(3):
                moved = window if k == 2 else pltpu.roll(window, 2 - k, 0)
                smoothed = smoothed + taps[k : k + 1, lo:hi] * moved[16:, :]
            hidden[rows(b), lo:hi] = (jax.nn.gelu(smoothed) * gated).astype(bf16)

        @pl.when(j == n_tp - 2)
        def _():
            w_step(2, 0)

        return 0

    lax.fori_loop(0, n_tp, gate_block, 0)
    w_local(2).wait()

    def shard_of(q):
        d = lax.div(q + 1, 2)
        return ring_chip(mod(place + jnp.where(lax.rem(q, 2) == 1, -d, d), n), nz, ny)

    others = list(range(1, nx)) + [0]

    def down_step(q, _):
        for k in range(1, n - 1):

            @pl.when(q == (k if k < n - 2 else n - 1))
            def _():
                w_step(2, k)

        @pl.when(q < n)
        def _():
            weight = down_full[:, columns(shard_of(q))]
            for dx in others:
                b = x_at(dx) + 1 - 2 * core
                made = jnp.dot(hidden[rows(b), :], weight, preferred_element_type=f32)
                gone(dx, q)[...] = made.astype(bf16)
                made = jnp.dot(hidden[rows(x_at(dx)), :], weight, preferred_element_type=f32)
                keep[dx, q] = made.astype(bf16)
                pc_copy(dx, q).start()
            for dx in range(1, nx):
                pc_copy(dx, q).wait_recv()
                both = keep[dx, q].astype(f32) + got_core[dx, q].astype(f32)
                keep[dx, q] = both.astype(bf16)
                px_copy(dx, q).start()

        @pl.when(q > 1)
        def _():
            p = q - 2
            f = shard_of(p)
            pc_copy(0, p).wait_recv()
            total = stream[:, columns(f)].astype(f32)
            total = total + keep[0, p].astype(f32) + got_core[0, p].astype(f32)
            for dx in range(1, nx):
                px_copy(dx, p).wait_recv()
                total = total + got_x[dx - 1, p].astype(f32)
            held[:, columns(f)] = total.astype(bf16)
            out_copy(f, p).start()

        return 0

    lax.fori_loop(0, n + 2, down_step, 0)

    def finish(q, _):
        out_copy(shard_of(q), q).wait()
        for dx in range(nx):
            pc_copy(dx, q).wait_send()
            if dx:
                px_copy(dx, q).wait_send()
        return 0

    lax.fori_loop(0, n, finish, 0)
    for dx in range(1, nx):
        t_copy(tp, tx_send.at[dx - 1], x_at(dx)).wait_send()
    for dx in range(nx):
        t_copy(x_at(dx), tc_send.at[dx], twin).wait_send()
    for m in range(3):
        w_drain(m)


def make_body(n_fs, n_tp, ny):
    nz, nx = n_fs // ny, n_tp // 2

    def body(
        mixed,
        residual,
        mix_weight,
        norm_gain,
        up_weight,
        gate_weight,
        conv_weight,
        conv_bias,
        down_weight,
    ):
        tok, width = residual.shape
        depth, (hid, wide) = mixed.shape[1], down_weight.shape
        dma = pltpu.SemaphoreType.DMA
        whole = pl.BlockSpec(memory_space=pl.ANY)
        small = pl.BlockSpec(memory_space=pltpu.VMEM)
        held = depth + 3 * hid + n_tp * tok + (3 * nx + 2) * tok
        lanes = (hid + 127) // 128 * 128
        held = held * width * 2 + n_tp * tok * lanes * 8 + (1 << 20)
        split = held <= VMEM
        return pl.pallas_call(
            functools.partial(layer_kernel, nz, ny, nx, split),
            out_shape=jax.ShapeDtypeStruct((tok, width), bf16),
            in_specs=[whole] * 6 + [small] * 3,
            out_specs=whole,
            scratch_shapes=[
                pltpu.VMEM((depth, width), bf16),
                pltpu.VMEM((hid, width), bf16),
                pltpu.VMEM((hid, width), bf16),
                pltpu.VMEM((hid, width), bf16),
                pltpu.VMEM((n_tp * tok, width), bf16),
                pltpu.VMEM((n_tp * tok + 16, hid), bf16),
                pltpu.VMEM((n_tp * tok, hid), bf16),
                pltpu.VMEM((n_tp * tok, hid) if split else (8, 128), f32),
                pltpu.VMEM((tok, depth), bf16),
                pltpu.VMEM((tok, width), bf16),
                pltpu.VMEM((tok, width), bf16),
                pltpu.VMEM((nx, n_fs, tok, wide), bf16),
                pltpu.VMEM((nx, n_fs, tok, wide), bf16),
                pltpu.VMEM((max(nx - 1, 1), n_fs, tok, wide), bf16),
                dma((3, 2, n_fs, 2)),
                dma((3, n_fs, 2)),
                dma((2, n_fs)),
                dma((n_fs, n_tp)),
                dma((2,)),
                dma((n_fs, max(nx - 1, 1))),
                dma((n_fs, nx)),
                dma((n_tp,)),
                dma((max(nx - 1, 1),)),
                dma((nx,)),
                dma((n_fs, nx)),
                dma((n_fs, nx)),
                dma((n_fs, max(nx - 1, 1))),
                dma((n_fs, max(nx - 1, 1))),
                dma((6,)),
                dma((n_fs,)),
            ],
            compiler_params=pltpu.CompilerParams(
                collective_id=0, has_side_effects=True, vmem_limit_bytes=VMEM
            ),
        )(
            mixed,
            residual,
            mix_weight,
            up_weight.T,
            gate_weight.T,
            down_weight,
            norm_gain[None, :],
            conv_weight,
            conv_bias,
        )

    return body


def solution(mesh):
    coords = [getattr(d, "coords", None) for d in mesh.devices[:, 0]]
    n_fs, n_tp = mesh.shape["fs"], mesh.shape["tp"]
    ny = len({c[1] for c in coords}) if None not in coords else 1
    if n_fs % ny:
        ny = 1
    return jax.shard_map(
        make_body(n_fs, n_tp, ny),
        mesh=mesh,
        in_specs=(
            P(("fs", "tp"), None),
            P(("fs", "tp"), None),
            P(("fs", "tp"), None),
            P(),
            P("fs", "tp"),
            P("fs", "tp"),
            P(None, "tp"),
            P("tp"),
            P("tp", "fs"),
        ),
        out_specs=P(("fs", "tp"), None),
        check_vma=False,
    )
```

```python
import functools

import jax
import jax.numpy as jnp
from jax import lax
from jax.experimental import pallas as pl
from jax.experimental.pallas import tpu as pltpu
from jax.sharding import PartitionSpec as P

norm_eps = 1e-06
f32, bf16 = jnp.float32, jnp.bfloat16
MESH = pl.DeviceIdType.MESH
NT = (((1,), (1,)), ((), ()))
TILE = 256
VMEM = 67043328


def mod(a, n):
    return lax.rem(a + n, n)


def ring_place(f, nz, ny):
    z, y = lax.div(f, ny), lax.rem(f, ny)
    if ny == 1:
        return z
    along = jnp.where(lax.rem(z, 2) == 0, y - 1, ny - 1 - y)
    return jnp.where(y == 0, nz * (ny - 1) + nz - 1 - z, z * (ny - 1) + along)


def ring_chip(r, nz, ny):
    if ny == 1:
        return r
    z, k = lax.div(r, ny - 1), lax.rem(r, ny - 1)
    out = z * ny + jnp.where(lax.rem(z, 2) == 0, 1 + k, ny - 1 - k)
    return jnp.where(r < nz * (ny - 1), out, (nz - 1 - (r - nz * (ny - 1))) * ny)


def layer_kernel(
    nz,
    ny,
    nx,
    split,
    mixed,
    residual,
    mix_shard,
    up_shard,
    gate_shard,
    down_shard,
    gain,
    taps,
    bias,
    held,
    mix_full,
    up_full,
    gate_full,
    down_full,
    tokens,
    up_part,
    hidden,
    gate_sum,
    mixed_v,
    stream,
    keep,
    got_core,
    got_x,
    w_send,
    w_recv,
    m_send,
    m_recv,
    end_recv,
    t_send,
    t_recv,
    p_send,
    pc_recv,
    px_recv,
    in_sem,
):
    n = nz * ny
    half_n = n // 2
    n_tp = 2 * nx
    me = lax.axis_index("fs")
    tp = lax.axis_index("tp")
    x, core = lax.div(tp, 2), lax.rem(tp, 2)
    place = ring_place(me, nz, ny)

    chips = [ring_chip(mod(place + d, n), nz, ny) for d in range(n)]

    def ring(d):
        return chips[d % n]

    nxt, prv = ring(1), ring(-1)
    twin = tp + 1 - 2 * core

    def x_at(dx):
        return lax.rem(x + dx, nx) * 2 + core

    tok, width = stream.shape
    hid, wide = up_shard.shape
    by_columns = wide % 256 == 0
    cut = wide // 2 if by_columns else (hid // 2 + 15) // 16 * 16
    halves = ((0, cut), (cut, (wide if by_columns else hid) - cut))
    fulls = (up_full, gate_full, down_full)
    shards = (up_shard, gate_shard, down_shard)
    n_step = n - 3
    mrows = mix_shard.shape[0]

    def remote(src, dst, send, recv, axis, to):
        return pltpu.make_async_remote_copy(
            src_ref=src,
            dst_ref=dst,
            send_sem=send,
            recv_sem=recv,
            device_id={axis: to},
            device_id_type=MESH,
        )

    def columns(f):
        return pl.ds(pl.multiple_of(f * wide, 128), wide)

    def slot(m, f, h):
        off, size = halves[h]
        if by_columns:
            return fulls[m].at[:, pl.ds(pl.multiple_of(f * wide + off, 128), size)]
        return fulls[m].at[pl.ds(off, size), columns(f)]

    def w_copy(m, f, h, way, mine=False):
        at = pl.ds(*halves[h])
        src = slot(m, f, h)
        if mine:
            src = shards[m].at[:, at] if by_columns else shards[m].at[at, :]
        to = prv if way else nxt
        return remote(src, slot(m, f, h), w_send.at[m], w_recv.at[m, f, h], "fs", to)

    def w_own(m):
        for k in range(2):
            w_copy(m, me, k, 0, True).start()
            w_copy(m, me, 1 - k, 1, True).start()

    def w_step(m, k):
        d, h = 1 + k // 2, k % 2
        for way, f, hh in ((0, ring(-d), h), (1, ring(d), 1 - h)):
            w_copy(m, f, hh, way).wait_recv()
            if k < n_step:
                w_copy(m, f, hh, way).start()

    def sent(ref, sem):
        remote(ref, ref, sem, sem, "fs", nxt).wait_send()

    def w_drain(m):
        sent(fulls[m].at[:, pl.ds(0, (n - 1) * wide)], w_send.at[m])

    def w_local(m):
        return pltpu.make_async_copy(shards[m], fulls[m].at[:, columns(me)], in_sem.at[m])

    def part(f, t):
        return mix_full.at[pl.ds(pl.multiple_of((f * n_tp + t) * mrows, 16), mrows), :]

    def m_ring(f, way, mine=False, last=False):
        src, dst = mix_shard if mine else part(f, tp), part(f, tp)
        to, got = prv if way else nxt, m_recv.at[f, 0]
        if last:
            cols = pl.ds(way * (width // 2), width // 2)
            src = dst = dst.at[:, cols]
            got = end_recv.at[way]
        return remote(src, dst, m_send.at[0], got, "fs", to)

    def m_x(f, dx, mine=False):
        src = mix_shard if mine else part(f, tp)
        return remote(src, part(f, tp), m_send.at[1], m_recv.at[f, dx], "tp", x_at(dx))

    def m_core(f, dx, mine=False):
        t = x_at(dx)
        src = mix_shard if mine else part(f, t)
        return remote(src, part(f, t), m_send.at[2], end_recv.at[2], "tp", twin)

    def m_spread(f, mine=False):
        for dx in range(1, nx):
            m_x(f, dx, mine).start()
        m_core(f, 0, mine).start()

    def m_wait(f, t, got):
        remote(part(f, t), part(f, t), m_send.at[2], got, "tp", twin).wait_recv()

    def m_step(d):
        if d == half_n:
            for way in range(2):
                m_ring(ring(d), way, last=True).wait_recv()
            m_spread(ring(d))
            return
        for way in range(2):
            f = ring(d if way else -d)
            m_wait(f, tp, m_recv.at[f, 0])
            m_ring(f, way, last=d == half_n - 1).start()
            m_spread(f)

    def m_relay(f):
        for dx in range(1, nx):
            m_wait(f, x_at(dx), m_recv.at[f, nx - dx])
            m_core(f, dx).start()

    def m_drain():
        for lane, count in enumerate((n - 1, n * (nx - 1), n * nx)):
            sent(mix_full.at[pl.ds(0, count * mrows), :], m_send.at[lane])

    def rows(b):
        return pl.ds(pl.multiple_of(b * tok, 16), tok)

    def t_copy(b, send, to):
        return remote(tokens.at[rows(b), :], tokens.at[rows(b), :], send, t_recv.at[b], "tp", to)

    def t_wait(b):
        t_copy(b, t_send.at[1], twin).wait_recv()

    def gone(dx, q):
        return mix_full.at[pl.ds(dx * tok, tok), columns(q)]

    def pc_copy(dx, q):
        return remote(
            gone(dx, q), got_core.at[dx, q], p_send.at[0], pc_recv.at[q, dx], "tp", twin
        )

    def px_copy(dx, q):
        return remote(
            keep.at[dx, q],
            got_x.at[dx - 1, q],
            p_send.at[1],
            px_recv.at[q, dx - 1],
            "tp",
            x_at(dx),
        )

    load_mixed = pltpu.make_async_copy(mixed, mixed_v, in_sem.at[3])
    load_residual = pltpu.make_async_copy(residual, held, in_sem.at[4])
    load_mix = pltpu.make_async_copy(mix_shard, part(me, tp), in_sem.at[5])

    barrier = pltpu.get_barrier_semaphore()
    for other in (nxt, prv):
        pl.semaphore_signal(barrier, inc=1, device_id={"fs": other}, device_id_type=MESH)
    for other in [twin] + [x_at(dx) for dx in range(1, nx)]:
        pl.semaphore_signal(barrier, inc=1, device_id={"tp": other}, device_id_type=MESH)
    pl.semaphore_wait(barrier, 2 + nx)

    m_ring(me, 0, True).start()
    m_ring(me, 1, True).start()
    m_spread(me, True)
    load_mix.start()
    load_mixed.start()
    load_residual.start()
    for m in range(3):
        w_local(m).start()
    up_part[0:16, :] = jnp.zeros((16, hid), bf16)

    early = min(n_step, half_n - 1)
    for d in range(1, half_n + 1):
        m_step(d)
        if d == 1:
            w_own(0)
        if 2 <= d < early + 2:
            w_step(0, d - 2)
    for q in range(n):
        d = (q + 1) // 2
        m_relay(ring(-d if q % 2 else d))
    from_twin = mix_full.at[pl.ds(0, n * nx * mrows), :]
    remote(from_twin, from_twin, m_send.at[2], end_recv.at[2], "tp", twin).wait_recv()
    load_mix.wait()
    load_mixed.wait()
    load_residual.wait()

    def project(i, _):
        cols = pl.ds(pl.multiple_of(i * TILE, 128), TILE)
        made = jnp.dot(mixed_v[...], mix_full[:, cols], preferred_element_type=f32)
        stream[:, cols] = (held[:, cols].astype(f32) + made).astype(bf16)
        return 0

    lax.fori_loop(0, width // TILE, project, 0)

    for k in range(early, min(early + 1, n_step)):
        w_step(0, k)

    def norm(i, _):
        at = pl.multiple_of(i * 32, 16)
        row = stream[pl.ds(at, 32), :].astype(f32)
        scale = lax.rsqrt(jnp.mean(row * row, axis=-1, keepdims=True) + norm_eps)
        tokens[pl.ds(pl.multiple_of(tp * tok + at, 16), 32), :] = (row * scale * gain[...]).astype(
            bf16
        )
        return 0

    lax.fori_loop(0, tok // 32, norm, 0)
    for dx in range(1, nx):
        t_copy(tp, t_send.at[0], x_at(dx)).start()
    t_copy(tp, t_send.at[1], twin).start()

    for k in range(min(early + 1, n_step), n_step):
        w_step(0, k)
    w_own(1)
    for k in range(n_step, n - 1):
        w_step(0, k)
    w_local(0).wait()

    def block_of(j):
        return lax.rem(x + lax.div(j, 2), nx) * 2 + lax.rem(core + lax.rem(j, 2), 2)

    def up_block(j, _):
        b = block_of(j)

        @pl.when(j > 0)
        def _():
            t_wait(b)

        @pl.when((j > 1) & (lax.rem(j, 2) == 0))
        def _():
            t_copy(b, t_send.at[1], twin).start()

        for lo in range(0, hid, TILE):
            hi = min(lo + TILE, hid)
            made = lax.dot_general(
                tokens[rows(b), :], up_full[lo:hi, :], NT, preferred_element_type=f32
            )
            up_part[pl.ds(pl.multiple_of(16 + b * tok, 16), tok), lo:hi] = made.astype(bf16)
        for at, ks in ((1, (0, 1)), (n_tp - 2, (2,))):
            for k in ks:
                if k < ahead:

                    @pl.when(j == at)
                    def _():
                        w_step(1, k)

        return 0

    ahead = min(3, n_step)
    lax.fori_loop(0, n_tp, up_block, 0)

    def gate_dot(b, lo, hi, fs):
        made = None
        for f in fs:
            term = lax.dot_general(
                tokens[rows(b), columns(f)],
                gate_full[lo:hi, columns(f)],
                NT,
                preferred_element_type=f32,
            )
            made = term if made is None else made + term
        return made

    def gate_pass(d):
        fs = ([me] if d == 1 else []) + [ring(-d), ring(d)]

        def add(b, _):
            for lo in range(0, hid, TILE):
                hi = min(lo + TILE, hid)
                made = gate_dot(b, lo, hi, fs)
                if d > 1:
                    made = gate_sum[rows(b), lo:hi] + made
                gate_sum[rows(b), lo:hi] = made
            return 0

        lax.fori_loop(0, n_tp, add, 0)

    w_local(1).wait()
    for d in range(1, half_n):
        for k in (2 * d - 2, 2 * d - 1):
            if k >= ahead:
                w_step(1, k)
            if k == n_step - 1:
                w_own(2)
        if split:
            gate_pass(d)
    w_step(1, n - 2)
    m_drain()
    for lane in range(2):
        sent(tokens.at[pl.ds(0, (nx - 1 + lane) * tok), :], t_send.at[lane])
    for m in range(2):
        w_drain(m)

    def gate_block(j, _):
        b = block_of(j)
        for lo in range(0, hid, TILE):
            hi = min(lo + TILE, hid)
            if split:
                made = gate_sum[rows(b), lo:hi] + gate_dot(b, lo, hi, [ring(half_n)])
            else:
                made = lax.dot_general(
                    tokens[rows(b), :], gate_full[lo:hi, :], NT, preferred_element_type=f32
                )
            gated = made.astype(bf16).astype(f32)
            window = up_part[pl.ds(pl.multiple_of(b * tok, 16), tok + 16), lo:hi].astype(f32)
            smoothed = bias[lo:hi][None, :]
            for k in range(3):
                moved = window if k == 2 else pltpu.roll(window, 2 - k, 0)
                smoothed = smoothed + taps[k : k + 1, lo:hi] * moved[16:, :]
            hidden[rows(b), lo:hi] = (jax.nn.gelu(smoothed) * gated).astype(bf16)

        @pl.when(j == n_tp - 2)
        def _():
            w_step(2, 0)

        return 0

    lax.fori_loop(0, n_tp, gate_block, 0)
    w_local(2).wait()

    def pieces(q):
        if not by_columns:
            d = lax.div(q + 1, 2)
            d = jnp.where(lax.rem(q, 2) == 1, -d, d)
            return [columns(ring_chip(mod(place + d, n), nz, ny))]
        k = jnp.maximum(q - 1, 0)
        d, h = jnp.where(q == 0, 0, 1 + lax.div(k, 2)), lax.rem(k, 2)
        left = ring_chip(mod(place - d, n), nz, ny) * wide + h * cut
        right = ring_chip(mod(place + d, n), nz, ny) * wide + (1 - h) * cut
        return [pl.ds(pl.multiple_of(at, 128), cut) for at in (left, right)]

    def step_at(k):
        return k + 1 if by_columns else k if k < n - 2 else n - 1

    others = list(range(1, nx)) + [0]

    def down_step(q, _):
        for k in range(1, n - 1):

            @pl.when(q == step_at(k))
            def _():
                w_step(2, k)

        @pl.when(q < n)
        def _():
            weight = jnp.concatenate([down_full[:, cols] for cols in pieces(q)], axis=1)
            for dx in others:
                b = x_at(dx) + 1 - 2 * core
                made = jnp.dot(hidden[rows(b), :], weight, preferred_element_type=f32)
                gone(dx, q)[...] = made.astype(bf16)
                made = jnp.dot(hidden[rows(x_at(dx)), :], weight, preferred_element_type=f32)
                keep[dx, q] = made.astype(bf16)
                pc_copy(dx, q).start()
            for dx in range(1, nx):
                pc_copy(dx, q).wait_recv()
                both = keep[dx, q].astype(f32) + got_core[dx, q].astype(f32)
                keep[dx, q] = both.astype(bf16)
                px_copy(dx, q).start()

        @pl.when(q > 1)
        def _():
            p = q - 2
            pc_copy(0, p).wait_recv()
            total = keep[0, p].astype(f32) + got_core[0, p].astype(f32)
            for dx in range(1, nx):
                px_copy(dx, p).wait_recv()
                total = total + got_x[dx - 1, p].astype(f32)
            off = 0
            for cols in pieces(p):
                size = cols.size
                whole = stream[:, cols].astype(f32) + total[:, off : off + size]
                held[:, cols] = whole.astype(bf16)
                off += size

        return 0

    lax.fori_loop(0, n + 2, down_step, 0)
    sent(mix_full.at[pl.ds(0, nx * tok), :], p_send.at[0])
    for dx in range(1, nx):
        sent(mix_full.at[pl.ds(0, tok), :], p_send.at[1])
    w_drain(2)


def make_body(n_fs, n_tp, ny):
    nz, nx = n_fs // ny, n_tp // 2

    def body(
        mixed,
        residual,
        mix_weight,
        norm_gain,
        up_weight,
        gate_weight,
        conv_weight,
        conv_bias,
        down_weight,
    ):
        tok, width = residual.shape
        depth, (hid, wide) = mixed.shape[1], down_weight.shape
        dma = pltpu.SemaphoreType.DMA
        whole = pl.BlockSpec(memory_space=pl.ANY)
        small = pl.BlockSpec(memory_space=pltpu.VMEM)
        held = depth + 3 * hid + n_tp * tok + (3 * nx + 2) * tok
        lanes = (hid + 127) // 128 * 128
        held = held * width * 2 + n_tp * tok * lanes * 8 + (1 << 20)
        split = held <= VMEM
        return pl.pallas_call(
            functools.partial(layer_kernel, nz, ny, nx, split),
            out_shape=pltpu.VMEM((tok, width), bf16),
            in_specs=[whole] * 6 + [small] * 3,
            out_specs=small,
            scratch_shapes=[
                pltpu.VMEM((depth, width), bf16),
                pltpu.VMEM((hid, width), bf16),
                pltpu.VMEM((hid, width), bf16),
                pltpu.VMEM((hid, width), bf16),
                pltpu.VMEM((n_tp * tok, width), bf16),
                pltpu.VMEM((n_tp * tok + 16, hid), bf16),
                pltpu.VMEM((n_tp * tok, hid), bf16),
                pltpu.VMEM((n_tp * tok, hid) if split else (8, 128), f32),
                pltpu.VMEM((tok, depth), bf16),
                pltpu.VMEM((tok, width), bf16),
                pltpu.VMEM((nx, n_fs, tok, wide), bf16),
                pltpu.VMEM((nx, n_fs, tok, wide), bf16),
                pltpu.VMEM((max(nx - 1, 1), n_fs, tok, wide), bf16),
                dma((3,)),
                dma((3, n_fs, 2)),
                dma((3,)),
                dma((n_fs, nx)),
                dma((3,)),
                dma((2,)),
                dma((n_tp,)),
                dma((2,)),
                dma((n_fs, nx)),
                dma((n_fs, max(nx - 1, 1))),
                dma((6,)),
            ],
            compiler_params=pltpu.CompilerParams(
                collective_id=0, has_side_effects=True, vmem_limit_bytes=VMEM - 2 * tok * width * 2
            ),
        )(
            mixed,
            residual,
            mix_weight,
            up_weight.T,
            gate_weight.T,
            down_weight,
            norm_gain[None, :],
            conv_weight,
            conv_bias,
        )

    return body


def solution(mesh):
    coords = [getattr(d, "coords", None) for d in mesh.devices[:, 0]]
    n_fs, n_tp = mesh.shape["fs"], mesh.shape["tp"]
    ny = len({c[1] for c in coords}) if None not in coords else 1
    if n_fs % ny:
        ny = 1
    return jax.shard_map(
        make_body(n_fs, n_tp, ny),
        mesh=mesh,
        in_specs=(
            P(("fs", "tp"), None),
            P(("fs", "tp"), None),
            P(("fs", "tp"), None),
            P(),
            P("fs", "tp"),
            P("fs", "tp"),
            P(None, "tp"),
            P("tp"),
            P("tp", "fs"),
        ),
        out_specs=P(("fs", "tp"), None),
        check_vma=False,
    )
```

```python
import functools

import jax
import jax.numpy as jnp
from jax import lax
from jax.experimental import pallas as pl
from jax.experimental.pallas import tpu as pltpu
from jax.sharding import PartitionSpec as P

norm_eps = 1e-06
f32, bf16 = jnp.float32, jnp.bfloat16
MESH = pl.DeviceIdType.MESH
NT = (((1,), (1,)), ((), ()))
TILE = 256
VMEM = 67043328


def mod(a, n):
    return lax.rem(a + n, n)


def ring_place(f, nz, ny):
    z, y = lax.div(f, ny), lax.rem(f, ny)
    if ny == 1:
        return z
    along = jnp.where(lax.rem(z, 2) == 0, y - 1, ny - 1 - y)
    return jnp.where(y == 0, nz * (ny - 1) + nz - 1 - z, z * (ny - 1) + along)


def ring_chip(r, nz, ny):
    if ny == 1:
        return r
    z, k = lax.div(r, ny - 1), lax.rem(r, ny - 1)
    out = z * ny + jnp.where(lax.rem(z, 2) == 0, 1 + k, ny - 1 - k)
    return jnp.where(r < nz * (ny - 1), out, (nz - 1 - (r - nz * (ny - 1))) * ny)


def layer_kernel(
    nz,
    ny,
    nx,
    split,
    mixed,
    residual,
    mix_shard,
    up_shard,
    gate_shard,
    down_shard,
    gain,
    taps,
    bias,
    held,
    mix_full,
    up_full,
    gate_full,
    down_full,
    tokens,
    up_part,
    hidden,
    gate_sum,
    mixed_v,
    stream,
    keep,
    got_core,
    got_x,
    w_send,
    w_recv,
    m_send,
    m_ring_recv,
    m_recv,
    m_core_recv,
    t_send,
    t_recv,
    p_send,
    pc_recv,
    px_recv,
    in_sem,
):
    n = nz * ny
    half_n = n // 2
    n_tp = 2 * nx
    me = lax.axis_index("fs")
    tp = lax.axis_index("tp")
    x, core = lax.div(tp, 2), lax.rem(tp, 2)
    place = ring_place(me, nz, ny)

    chips = [ring_chip(mod(place + d, n), nz, ny) for d in range(n)]

    def ring(d):
        return chips[d % n]

    nxt, prv = ring(1), ring(-1)
    twin = tp + 1 - 2 * core

    def x_at(dx):
        return lax.rem(x + dx, nx) * 2 + core

    tok, width = stream.shape
    hid, wide = up_shard.shape
    by_columns = wide % 256 == 0
    cut = wide // 2 if by_columns else (hid // 2 + 15) // 16 * 16
    halves = ((0, cut), (cut, (wide if by_columns else hid) - cut))
    fulls = (up_full, gate_full, down_full)
    shards = (up_shard, gate_shard, down_shard)
    n_step = n - 3
    mrows = mix_shard.shape[0]
    front = width // 2
    mix_cut = ((0, front), (front, width - front))
    n_piece, piece = keep.shape[1], keep.shape[3]

    def remote(src, dst, send, recv, axis, to):
        return pltpu.make_async_remote_copy(
            src_ref=src,
            dst_ref=dst,
            send_sem=send,
            recv_sem=recv,
            device_id={axis: to},
            device_id_type=MESH,
        )

    def columns(f):
        return pl.ds(pl.multiple_of(f * wide, 128), wide)

    def slot(m, f, h):
        off, size = halves[h]
        if by_columns:
            return fulls[m].at[:, pl.ds(pl.multiple_of(f * wide + off, 128), size)]
        return fulls[m].at[pl.ds(off, size), columns(f)]

    def w_copy(m, f, h, way, mine=False):
        at = pl.ds(*halves[h])
        src = slot(m, f, h)
        if mine:
            src = shards[m].at[:, at] if by_columns else shards[m].at[at, :]
        to = prv if way else nxt
        return remote(src, slot(m, f, h), w_send.at[m], w_recv.at[m, f, h], "fs", to)

    def w_own(m):
        for k in range(2):
            w_copy(m, me, k, 0, True).start()
            w_copy(m, me, 1 - k, 1, True).start()

    def w_step(m, k, ways=(0, 1)):
        d = 1 + k // 2
        for way in ways:
            f, hh = (ring(d), 1 - k % 2) if way else (ring(-d), k % 2)
            w_copy(m, f, hh, way).wait_recv()
            if k < n_step:
                w_copy(m, f, hh, way).start()

    def sent(ref, sem):
        remote(ref, ref, sem, sem, "fs", nxt).wait_send()

    def w_drain(m):
        sent(fulls[m].at[:, pl.ds(0, (n - 1) * wide)], w_send.at[m])

    def w_local(m):
        return pltpu.make_async_copy(shards[m], fulls[m].at[:, columns(me)], in_sem.at[m])

    def part(f, t):
        return mix_full.at[pl.ds(pl.multiple_of((f * n_tp + t) * mrows, 16), mrows), :]

    def m_half(f, h):
        return part(f, tp).at[:, pl.ds(*mix_cut[h])]

    def m_ring(f, h, way, mine=False):
        src = m_half(f, h)
        if mine:
            src = mix_shard.at[:, pl.ds(*mix_cut[h])]
        to = prv if way else nxt
        return remote(src, m_half(f, h), m_send.at[0], m_ring_recv.at[f, h], "fs", to)

    def m_x(f, dx, mine=False):
        src = mix_shard if mine else part(f, tp)
        return remote(src, part(f, tp), m_send.at[1], m_recv.at[f, dx - 1], "tp", x_at(dx))

    def m_core(f, dx, mine=False):
        t = x_at(dx)
        src = mix_shard if mine else part(f, t)
        return remote(src, part(f, t), m_send.at[2], m_core_recv.at[0], "tp", twin)

    def m_spread(f, mine=False):
        for dx in range(1, nx):
            m_x(f, dx, mine).start()
        m_core(f, 0, mine).start()

    def m_wait(f, t, got):
        remote(part(f, t), part(f, t), m_send.at[2], got, "tp", twin).wait_recv()

    def m_own():
        for k in range(2):
            m_ring(me, k, 0, True).start()
            m_ring(me, 1 - k, 1, True).start()

    def m_step(d):
        for k in (2 * d - 2, 2 * d - 1):
            for way, f, h in ((0, ring(-d), k % 2), (1, ring(d), 1 - k % 2)):
                if k < n - 1:
                    m_ring(f, h, way).wait_recv()
                if k < n_step:
                    m_ring(f, h, way).start()
        for f in (ring(-d), ring(d)) if d < half_n else (ring(d),):
            m_spread(f)

    def m_relay(f):
        for dx in range(1, nx):
            m_wait(f, x_at(dx), m_recv.at[f, nx - dx - 1])
            m_core(f, dx).start()

    def m_drain():
        for lane, count in enumerate((n - 1, n * (nx - 1), n * nx)):
            sent(mix_full.at[pl.ds(0, count * mrows), :], m_send.at[lane])

    def rows(b):
        return pl.ds(pl.multiple_of(b * tok, 16), tok)

    def t_copy(b, send, to):
        return remote(tokens.at[rows(b), :], tokens.at[rows(b), :], send, t_recv.at[b], "tp", to)

    def t_wait(b):
        t_copy(b, t_send.at[1], twin).wait_recv()

    def gone(dx, q):
        at = pl.multiple_of(q * piece, 128)
        return mix_full.at[pl.ds(dx * tok, tok), pl.ds(at, piece)]

    def pc_copy(dx, q):
        return remote(
            gone(dx, q), got_core.at[dx, q], p_send.at[0], pc_recv.at[q, dx], "tp", twin
        )

    def px_copy(dx, q):
        src, dst = keep.at[dx, q], got_x.at[dx - 1, q]
        return remote(src, dst, p_send.at[1], px_recv.at[q, dx - 1], "tp", x_at(dx))

    load_mixed = pltpu.make_async_copy(mixed, mixed_v, in_sem.at[3])
    load_residual = pltpu.make_async_copy(residual, held, in_sem.at[4])
    load_mix = pltpu.make_async_copy(mix_shard, part(me, tp), in_sem.at[5])

    barrier = pltpu.get_barrier_semaphore()
    for other in (nxt, prv):
        pl.semaphore_signal(barrier, inc=1, device_id={"fs": other}, device_id_type=MESH)
    for other in [twin] + [x_at(dx) for dx in range(1, nx)]:
        pl.semaphore_signal(barrier, inc=1, device_id={"tp": other}, device_id_type=MESH)
    pl.semaphore_wait(barrier, 2 + nx)

    m_own()
    m_spread(me, True)
    load_mix.start()
    load_mixed.start()
    load_residual.start()
    for m in range(3):
        w_local(m).start()
    up_part[0:16, :] = jnp.zeros((16, hid), bf16)

    early = min(n_step, half_n - 1)
    for d in range(1, half_n + 1):
        m_step(d)
        if d == 1:
            w_own(0)
        if 2 <= d < early + 2:
            w_step(0, d - 2)
    for q in range(n):
        d = (q + 1) // 2
        m_relay(ring(-d if q % 2 else d))
    from_twin = mix_full.at[pl.ds(0, n * nx * mrows), :]
    remote(from_twin, from_twin, m_send.at[2], m_core_recv.at[0], "tp", twin).wait_recv()
    load_mix.wait()
    load_mixed.wait()
    load_residual.wait()

    def project(i, _):
        cols = pl.ds(pl.multiple_of(i * TILE, 128), TILE)
        made = jnp.dot(mixed_v[...], mix_full[:, cols], preferred_element_type=f32)
        stream[:, cols] = (held[:, cols].astype(f32) + made).astype(bf16)
        return 0

    lax.fori_loop(0, width // TILE, project, 0)

    for k in range(early, min(early + 1, n_step)):
        w_step(0, k)

    def norm(i, _):
        at = pl.multiple_of(i * 32, 16)
        row = stream[pl.ds(at, 32), :].astype(f32)
        scale = lax.rsqrt(jnp.mean(row * row, axis=-1, keepdims=True) + norm_eps)
        tokens[pl.ds(pl.multiple_of(tp * tok + at, 16), 32), :] = (row * scale * gain[...]).astype(
            bf16
        )
        return 0

    lax.fori_loop(0, tok // 32, norm, 0)
    for dx in range(1, nx):
        t_copy(tp, t_send.at[0], x_at(dx)).start()
    t_copy(tp, t_send.at[1], twin).start()

    for k in range(min(early + 1, n_step), n_step):
        w_step(0, k)
    w_own(1)
    for k in range(n_step, n - 1):
        w_step(0, k)
    w_local(0).wait()

    def block_of(j):
        return lax.rem(x + lax.div(j, 2), nx) * 2 + lax.rem(core + lax.rem(j, 2), 2)

    def up_block(j, _):
        b = block_of(j)

        @pl.when(j > 0)
        def _():
            t_wait(b)

        @pl.when((j > 1) & (lax.rem(j, 2) == 0))
        def _():
            t_copy(b, t_send.at[1], twin).start()

        for lo in range(0, hid, TILE):
            hi = min(lo + TILE, hid)
            made = lax.dot_general(
                tokens[rows(b), :], up_full[lo:hi, :], NT, preferred_element_type=f32
            )
            up_part[pl.ds(pl.multiple_of(16 + b * tok, 16), tok), lo:hi] = made.astype(bf16)
        for at, ks in ((1, (0, 1)), (n_tp - 2, (2,))):
            for k in ks:
                if k < ahead:

                    @pl.when(j == at)
                    def _():
                        w_step(1, k)

        return 0

    ahead = min(3, n_step)
    lax.fori_loop(0, n_tp, up_block, 0)

    def gate_dot(b, lo, hi, fs):
        made = None
        for f in fs:
            term = lax.dot_general(
                tokens[rows(b), columns(f)],
                gate_full[lo:hi, columns(f)],
                NT,
                preferred_element_type=f32,
            )
            made = term if made is None else made + term
        return made

    def gate_pass(d):
        fs = ([me] if d == 1 else []) + [ring(-d), ring(d)]

        def add(b, _):
            for lo in range(0, hid, TILE):
                hi = min(lo + TILE, hid)
                made = gate_dot(b, lo, hi, fs)
                if d > 1:
                    made = gate_sum[rows(b), lo:hi] + made
                gate_sum[rows(b), lo:hi] = made
            return 0

        lax.fori_loop(0, n_tp, add, 0)

    w_local(1).wait()
    for d in range(1, half_n):
        for k in (2 * d - 2, 2 * d - 1):
            if k >= ahead:
                w_step(1, k)
            if k == n_step - 1:
                w_own(2)
        if split:
            gate_pass(d)
    w_step(1, n - 2)
    m_drain()
    for lane in range(2):
        sent(tokens.at[pl.ds(0, (nx - 1 + lane) * tok), :], t_send.at[lane])
    for m in range(2):
        w_drain(m)

    def gate_block(j, _):
        b = block_of(j)
        for lo in range(0, hid, TILE):
            hi = min(lo + TILE, hid)
            if split:
                made = gate_sum[rows(b), lo:hi] + gate_dot(b, lo, hi, [ring(half_n)])
            else:
                made = lax.dot_general(
                    tokens[rows(b), :], gate_full[lo:hi, :], NT, preferred_element_type=f32
                )
            gated = made.astype(bf16).astype(f32)
            window = up_part[pl.ds(pl.multiple_of(b * tok, 16), tok + 16), lo:hi].astype(f32)
            smoothed = bias[lo:hi][None, :]
            for k in range(3):
                moved = window if k == 2 else pltpu.roll(window, 2 - k, 0)
                smoothed = smoothed + taps[k : k + 1, lo:hi] * moved[16:, :]
            hidden[rows(b), lo:hi] = (jax.nn.gelu(smoothed) * gated).astype(bf16)

        @pl.when(j == n_tp - 2)
        def _():
            w_step(2, 0)

        return 0

    lax.fori_loop(0, n_tp, gate_block, 0)
    w_local(2).wait()

    def piece_columns(q):
        if by_columns:
            k, way = lax.div(jnp.maximum(q - 2, 0), 2), lax.rem(q, 2)
            d = jnp.where(q < 2, 0, 1 + lax.div(k, 2))
            h = jnp.where(way == 0, lax.rem(k, 2), 1 - lax.rem(k, 2))
        else:
            d, h, way = lax.div(q + 1, 2), 0, 1 - lax.rem(q, 2)
        f = ring_chip(mod(place + jnp.where(way == 0, -d, d), n), nz, ny)
        return pl.ds(pl.multiple_of(f * wide + h * piece, 128), piece)

    def steps_before(q):
        if by_columns:
            k = (q - 2) // 2
            return [(k, (q % 2,))] if 0 < k else []
        ks = [n - 2] if q == n - 1 else [q] if 0 < q < n - 2 else []
        return [(k, (0, 1)) for k in ks]

    def product(q, b):
        made = jnp.dot(
            hidden[rows(b), :], down_full[:, piece_columns(q)], preferred_element_type=f32
        )
        return made.astype(bf16)

    def make(q, dx):
        gone(dx, q)[...] = product(q, x_at(dx) + 1 - 2 * core)
        keep[dx, q] = product(q, x_at(dx))
        pc_copy(dx, q).start()

    def make_far(q):
        for dx in range(1, nx):
            make(q, dx)

    def pair_far(q):
        for dx in range(1, nx):
            pc_copy(dx, q).wait_recv()
            both = keep[dx, q].astype(f32) + got_core[dx, q].astype(f32)
            keep[dx, q] = both.astype(bf16)
            px_copy(dx, q).start()

    def finish(q):
        cols = piece_columns(q)
        pc_copy(0, q).wait_recv()
        total = stream[:, cols].astype(f32) + keep[0, q].astype(f32)
        total = total + got_core[0, q].astype(f32)
        for dx in range(1, nx):
            px_copy(dx, q).wait_recv()
            total = total + got_x[dx - 1, q].astype(f32)
        held[:, cols] = total.astype(bf16)

    def down_step(q, _):
        for at in range(n_piece - 2):
            for k, ways in steps_before(at):

                @pl.when(q == at)
                def _():
                    w_step(2, k, ways)

        make_far(q)
        make(q, 0)
        pair_far(q)

        @pl.when(q > 1)
        def _():
            finish(q - 2)

        return 0

    lax.fori_loop(0, n_piece - 2, down_step, 0)
    last = (n_piece - 2, n_piece - 1)
    for q in last:
        for k, ways in steps_before(q):
            w_step(2, k, ways)
        make_far(q)
    for q in last:
        pair_far(q)
        make(q, 0)
    for q in range(n_piece - 4, n_piece):
        finish(q)
    sent(mix_full.at[pl.ds(0, nx * tok), :], p_send.at[0])
    for dx in range(1, nx):
        sent(mix_full.at[pl.ds(0, tok), :], p_send.at[1])
    w_drain(2)


def make_body(n_fs, n_tp, ny):
    nz, nx = n_fs // ny, n_tp // 2

    def body(
        mixed,
        residual,
        mix_weight,
        norm_gain,
        up_weight,
        gate_weight,
        conv_weight,
        conv_bias,
        down_weight,
    ):
        tok, width = residual.shape
        depth, (hid, wide) = mixed.shape[1], down_weight.shape
        piece = wide // 2 if wide % 256 == 0 else wide
        n_piece = width // piece
        dma = pltpu.SemaphoreType.DMA
        whole = pl.BlockSpec(memory_space=pl.ANY)
        small = pl.BlockSpec(memory_space=pltpu.VMEM)
        held = depth + 3 * hid + n_tp * tok + (3 * nx + 2) * tok
        lanes = (hid + 127) // 128 * 128
        held = held * width * 2 + n_tp * tok * lanes * 8 + (1 << 20)
        split = held <= VMEM
        return pl.pallas_call(
            functools.partial(layer_kernel, nz, ny, nx, split),
            out_shape=pltpu.VMEM((tok, width), bf16),
            in_specs=[whole] * 6 + [small] * 3,
            out_specs=small,
            scratch_shapes=[
                pltpu.VMEM((depth, width), bf16),
                pltpu.VMEM((hid, width), bf16),
                pltpu.VMEM((hid, width), bf16),
                pltpu.VMEM((hid, width), bf16),
                pltpu.VMEM((n_tp * tok, width), bf16),
                pltpu.VMEM((n_tp * tok + 16, hid), bf16),
                pltpu.VMEM((n_tp * tok, hid), bf16),
                pltpu.VMEM((n_tp * tok, hid) if split else (8, 128), f32),
                pltpu.VMEM((tok, depth), bf16),
                pltpu.VMEM((tok, width), bf16),
                pltpu.VMEM((nx, n_piece, tok, piece), bf16),
                pltpu.VMEM((nx, n_piece, tok, piece), bf16),
                pltpu.VMEM((max(nx - 1, 1), n_piece, tok, piece), bf16),
                dma((3,)),
                dma((3, n_fs, 2)),
                dma((3,)),
                dma((n_fs, 2)),
                dma((n_fs, max(nx - 1, 1))),
                dma((1,)),
                dma((2,)),
                dma((n_tp,)),
                dma((2,)),
                dma((n_piece, nx)),
                dma((n_piece, max(nx - 1, 1))),
                dma((6,)),
            ],
            compiler_params=pltpu.CompilerParams(
                collective_id=0, has_side_effects=True, vmem_limit_bytes=VMEM - 2 * tok * width * 2
            ),
        )(
            mixed,
            residual,
            mix_weight,
            up_weight.T,
            gate_weight.T,
            down_weight,
            norm_gain[None, :],
            conv_weight,
            conv_bias,
        )

    return body


def solution(mesh):
    coords = [getattr(d, "coords", None) for d in mesh.devices[:, 0]]
    n_fs, n_tp = mesh.shape["fs"], mesh.shape["tp"]
    ny = len({c[1] for c in coords}) if None not in coords else 1
    if n_fs % ny:
        ny = 1
    return jax.shard_map(
        make_body(n_fs, n_tp, ny),
        mesh=mesh,
        in_specs=(
            P(("fs", "tp"), None),
            P(("fs", "tp"), None),
            P(("fs", "tp"), None),
            P(),
            P("fs", "tp"),
            P("fs", "tp"),
            P(None, "tp"),
            P("tp"),
            P("tp", "fs"),
        ),
        out_specs=P(("fs", "tp"), None),
        check_vma=False,
    )
```

```python
import functools

import jax
import jax.numpy as jnp
from jax import lax
from jax.experimental import pallas as pl
from jax.experimental.pallas import tpu as pltpu
from jax.sharding import PartitionSpec as P

norm_eps = 1e-06
f32, bf16 = jnp.float32, jnp.bfloat16
MESH = pl.DeviceIdType.MESH
NT = (((1,), (1,)), ((), ()))
TILE = 256
VMEM = 67043328


def mod(a, n):
    return lax.rem(a + n, n)


def ring_place(f, nz, ny):
    z, y = lax.div(f, ny), lax.rem(f, ny)
    if ny == 1:
        return z
    along = jnp.where(lax.rem(z, 2) == 0, y - 1, ny - 1 - y)
    return jnp.where(y == 0, nz * (ny - 1) + nz - 1 - z, z * (ny - 1) + along)


def ring_chip(r, nz, ny):
    if ny == 1:
        return r
    z, k = lax.div(r, ny - 1), lax.rem(r, ny - 1)
    out = z * ny + jnp.where(lax.rem(z, 2) == 0, 1 + k, ny - 1 - k)
    return jnp.where(r < nz * (ny - 1), out, (nz - 1 - (r - nz * (ny - 1))) * ny)


def layer_kernel(
    nz,
    ny,
    nx,
    split,
    mixed,
    residual,
    mix_shard,
    up_shard,
    gate_shard,
    down_shard,
    gain_in,
    taps_in,
    bias_in,
    held,
    gain,
    taps,
    bias,
    mix_full,
    up_full,
    gate_full,
    down_full,
    tokens,
    up_part,
    hidden,
    gate_sum,
    mixed_v,
    stream,
    keep,
    got_core,
    got_x,
    w_send,
    w_recv,
    m_send,
    m_ring_recv,
    m_recv,
    m_core_recv,
    t_send,
    t_recv,
    p_send,
    pc_recv,
    px_recv,
    in_sem,
):
    n = nz * ny
    half_n = n // 2
    n_tp = 2 * nx
    me = lax.axis_index("fs")
    tp = lax.axis_index("tp")
    x, core = lax.div(tp, 2), lax.rem(tp, 2)
    place = ring_place(me, nz, ny)

    chips = [ring_chip(mod(place + d, n), nz, ny) for d in range(n)]

    def ring(d):
        return chips[d % n]

    nxt, prv = ring(1), ring(-1)
    twin = tp + 1 - 2 * core

    def x_at(dx):
        return lax.rem(x + dx, nx) * 2 + core

    tok, width = stream.shape
    hid, wide = up_shard.shape
    by_columns = wide % 256 == 0
    cut = wide // 2 if by_columns else (hid // 2 + 15) // 16 * 16
    halves = ((0, cut), (cut, (wide if by_columns else hid) - cut))
    fulls = (up_full, gate_full, down_full)
    shards = (up_shard, gate_shard, down_shard)
    n_step = n - 3
    mrows = mix_shard.shape[0]
    front = width // 2
    mix_cut = ((0, front), (front, width - front))
    n_piece, piece = keep.shape[1], keep.shape[3]

    def remote(src, dst, send, recv, axis, to):
        return pltpu.make_async_remote_copy(
            src_ref=src,
            dst_ref=dst,
            send_sem=send,
            recv_sem=recv,
            device_id={axis: to},
            device_id_type=MESH,
        )

    def columns(f):
        return pl.ds(pl.multiple_of(f * wide, 128), wide)

    def slot(m, f, h):
        off, size = halves[h]
        if by_columns:
            return fulls[m].at[:, pl.ds(pl.multiple_of(f * wide + off, 128), size)]
        return fulls[m].at[pl.ds(off, size), columns(f)]

    def w_copy(m, f, h, way, mine=False):
        at = pl.ds(*halves[h])
        src = slot(m, f, h)
        if mine:
            src = shards[m].at[:, at] if by_columns else shards[m].at[at, :]
        to = prv if way else nxt
        return remote(src, slot(m, f, h), w_send.at[m], w_recv.at[m, f, h], "fs", to)

    def w_own(m):
        for k in range(2):
            w_copy(m, me, k, 0, True).start()
            w_copy(m, me, 1 - k, 1, True).start()

    def w_step(m, k, ways=(0, 1)):
        d = 1 + k // 2
        for way in ways:
            f, hh = (ring(d), 1 - k % 2) if way else (ring(-d), k % 2)
            w_copy(m, f, hh, way).wait_recv()
            if k < n_step:
                w_copy(m, f, hh, way).start()

    def sent(ref, sem):
        remote(ref, ref, sem, sem, "fs", nxt).wait_send()

    def w_drain(m):
        sent(fulls[m].at[:, pl.ds(0, (n - 1) * wide)], w_send.at[m])

    def w_local(m):
        return pltpu.make_async_copy(shards[m], fulls[m].at[:, columns(me)], in_sem.at[m])

    def part(f, t):
        return mix_full.at[pl.ds(pl.multiple_of((f * n_tp + t) * mrows, 16), mrows), :]

    def m_half(f, h):
        return part(f, tp).at[:, pl.ds(*mix_cut[h])]

    def m_ring(f, h, way, mine=False):
        src = m_half(f, h)
        if mine:
            src = mix_shard.at[:, pl.ds(*mix_cut[h])]
        to = prv if way else nxt
        return remote(src, m_half(f, h), m_send.at[0], m_ring_recv.at[f, h], "fs", to)

    def m_x(f, dx, mine=False):
        src = mix_shard if mine else part(f, tp)
        return remote(src, part(f, tp), m_send.at[1], m_recv.at[f, dx - 1], "tp", x_at(dx))

    def m_core(f, dx, mine=False):
        t = x_at(dx)
        src = mix_shard if mine else part(f, t)
        return remote(src, part(f, t), m_send.at[2], m_core_recv.at[0], "tp", twin)

    def m_spread(f, mine=False):
        for dx in range(1, nx):
            m_x(f, dx, mine).start()
        m_core(f, 0, mine).start()

    def m_wait(f, t, got):
        remote(part(f, t), part(f, t), m_send.at[2], got, "tp", twin).wait_recv()

    def m_own():
        for k in range(2):
            m_ring(me, k, 0, True).start()
            m_ring(me, 1 - k, 1, True).start()

    def m_step(d):
        for k in (2 * d - 2, 2 * d - 1):
            for way, f, h in ((0, ring(-d), k % 2), (1, ring(d), 1 - k % 2)):
                if k < n - 1:
                    m_ring(f, h, way).wait_recv()
                if k < n_step:
                    m_ring(f, h, way).start()
        for f in (ring(-d), ring(d)) if d < half_n else (ring(d),):
            m_spread(f)

    def m_relay(f):
        for dx in range(1, nx):
            m_wait(f, x_at(dx), m_recv.at[f, nx - dx - 1])
            m_core(f, dx).start()

    def m_drain():
        for lane, count in enumerate((n - 1, n * (nx - 1), n * nx)):
            sent(mix_full.at[pl.ds(0, count * mrows), :], m_send.at[lane])

    def rows(b):
        return pl.ds(pl.multiple_of(b * tok, 16), tok)

    def t_copy(b, send, to):
        return remote(tokens.at[rows(b), :], tokens.at[rows(b), :], send, t_recv.at[b], "tp", to)

    def t_wait(b):
        t_copy(b, t_send.at[1], twin).wait_recv()

    def gone(dx, q):
        at = pl.multiple_of(q * piece, 128)
        return mix_full.at[pl.ds(dx * tok, tok), pl.ds(at, piece)]

    def pc_copy(dx, q):
        return remote(
            gone(dx, q), got_core.at[dx, q], p_send.at[0], pc_recv.at[q, dx], "tp", twin
        )

    def px_copy(dx, q):
        src, dst = keep.at[dx, q], got_x.at[dx - 1, q]
        return remote(src, dst, p_send.at[1], px_recv.at[q, dx - 1], "tp", x_at(dx))

    load_mixed = pltpu.make_async_copy(mixed, mixed_v, in_sem.at[3])
    load_residual = pltpu.make_async_copy(residual, held, in_sem.at[4])
    load_mix = pltpu.make_async_copy(mix_shard, part(me, tp), in_sem.at[5])
    small_loads = [
        pltpu.make_async_copy(src, dst, in_sem.at[6 + i])
        for i, (src, dst) in enumerate(((gain_in, gain), (taps_in, taps), (bias_in, bias)))
    ]

    barrier = pltpu.get_barrier_semaphore()
    for other in (nxt, prv):
        pl.semaphore_signal(barrier, inc=1, device_id={"fs": other}, device_id_type=MESH)
    for other in [twin] + [x_at(dx) for dx in range(1, nx)]:
        pl.semaphore_signal(barrier, inc=1, device_id={"tp": other}, device_id_type=MESH)
    pl.semaphore_wait(barrier, 2 + nx)

    m_own()
    m_spread(me, True)
    load_mix.start()
    load_mixed.start()
    load_residual.start()
    for load in small_loads:
        load.start()
    for m in range(3):
        w_local(m).start()
    up_part[0:16, :] = jnp.zeros((16, hid), bf16)

    early = min(n_step, half_n - 1)
    for d in range(1, half_n + 1):
        m_step(d)
        if d == 1:
            w_own(0)
        if 2 <= d < early + 2:
            w_step(0, d - 2)
    for q in range(n):
        d = (q + 1) // 2
        m_relay(ring(-d if q % 2 else d))
    from_twin = mix_full.at[pl.ds(0, n * nx * mrows), :]
    remote(from_twin, from_twin, m_send.at[2], m_core_recv.at[0], "tp", twin).wait_recv()
    load_mix.wait()
    load_mixed.wait()
    load_residual.wait()
    for load in small_loads:
        load.wait()

    def project(i, _):
        cols = pl.ds(pl.multiple_of(i * TILE, 128), TILE)
        made = jnp.dot(mixed_v[...], mix_full[:, cols], preferred_element_type=f32)
        stream[:, cols] = (held[:, cols].astype(f32) + made).astype(bf16)
        return 0

    lax.fori_loop(0, width // TILE, project, 0)

    for k in range(early, min(early + 1, n_step)):
        w_step(0, k)

    def norm(i, _):
        at = pl.multiple_of(i * 32, 16)
        row = stream[pl.ds(at, 32), :].astype(f32)
        scale = lax.rsqrt(jnp.mean(row * row, axis=-1, keepdims=True) + norm_eps)
        tokens[pl.ds(pl.multiple_of(tp * tok + at, 16), 32), :] = (row * scale * gain[...]).astype(
            bf16
        )
        return 0

    lax.fori_loop(0, tok // 32, norm, 0)
    for dx in range(1, nx):
        t_copy(tp, t_send.at[0], x_at(dx)).start()
    t_copy(tp, t_send.at[1], twin).start()

    for k in range(min(early + 1, n_step), n_step):
        w_step(0, k)
    w_own(1)
    for k in range(n_step, n - 1):
        w_step(0, k)
    w_local(0).wait()

    def block_of(j):
        return lax.rem(x + lax.div(j, 2), nx) * 2 + lax.rem(core + lax.rem(j, 2), 2)

    def up_block(j, _):
        b = block_of(j)

        @pl.when(j > 0)
        def _():
            t_wait(b)

        @pl.when((j > 1) & (lax.rem(j, 2) == 0))
        def _():
            t_copy(b, t_send.at[1], twin).start()

        for lo in range(0, hid, TILE):
            hi = min(lo + TILE, hid)
            made = lax.dot_general(
                tokens[rows(b), :], up_full[lo:hi, :], NT, preferred_element_type=f32
            )
            up_part[pl.ds(pl.multiple_of(16 + b * tok, 16), tok), lo:hi] = made.astype(bf16)
        for at, ks in ((1, (0, 1)), (n_tp - 2, (2,))):
            for k in ks:
                if k < ahead:

                    @pl.when(j == at)
                    def _():
                        w_step(1, k)

        return 0

    ahead = min(3, n_step)
    lax.fori_loop(0, n_tp, up_block, 0)

    def gate_dot(b, lo, hi, fs):
        made = None
        for f in fs:
            term = lax.dot_general(
                tokens[rows(b), columns(f)],
                gate_full[lo:hi, columns(f)],
                NT,
                preferred_element_type=f32,
            )
            made = term if made is None else made + term
        return made

    def gate_pass(d):
        fs = ([me] if d == 1 else []) + [ring(-d), ring(d)]

        def add(b, _):
            for lo in range(0, hid, TILE):
                hi = min(lo + TILE, hid)
                made = gate_dot(b, lo, hi, fs)
                if d > 1:
                    made = gate_sum[rows(b), lo:hi] + made
                gate_sum[rows(b), lo:hi] = made
            return 0

        lax.fori_loop(0, n_tp, add, 0)

    w_local(1).wait()
    for d in range(1, half_n):
        for k in (2 * d - 2, 2 * d - 1):
            if k >= ahead:
                w_step(1, k)
            if k == n_step - 1:
                w_own(2)
        if split:
            gate_pass(d)
    w_step(1, n - 2)
    m_drain()
    for lane in range(2):
        sent(tokens.at[pl.ds(0, (nx - 1 + lane) * tok), :], t_send.at[lane])
    for m in range(2):
        w_drain(m)

    def gate_block(j, _):
        b = block_of(j)
        for lo in range(0, hid, TILE):
            hi = min(lo + TILE, hid)
            if split:
                made = gate_sum[rows(b), lo:hi] + gate_dot(b, lo, hi, [ring(half_n)])
            else:
                made = lax.dot_general(
                    tokens[rows(b), :], gate_full[lo:hi, :], NT, preferred_element_type=f32
                )
            gated = made.astype(bf16).astype(f32)
            window = up_part[pl.ds(pl.multiple_of(b * tok, 16), tok + 16), lo:hi].astype(f32)
            smoothed = bias[lo:hi][None, :]
            for k in range(3):
                moved = window if k == 2 else pltpu.roll(window, 2 - k, 0)
                smoothed = smoothed + taps[k : k + 1, lo:hi] * moved[16:, :]
            hidden[rows(b), lo:hi] = (jax.nn.gelu(smoothed) * gated).astype(bf16)

        @pl.when(j == n_tp - 2)
        def _():
            w_step(2, 0)

        return 0

    lax.fori_loop(0, n_tp, gate_block, 0)
    w_local(2).wait()

    def piece_columns(q):
        if by_columns:
            k, way = lax.div(jnp.maximum(q - 2, 0), 2), lax.rem(q, 2)
            d = jnp.where(q < 2, 0, 1 + lax.div(k, 2))
            h = jnp.where(way == 0, lax.rem(k, 2), 1 - lax.rem(k, 2))
        else:
            d, h, way = lax.div(q + 1, 2), 0, 1 - lax.rem(q, 2)
        f = ring_chip(mod(place + jnp.where(way == 0, -d, d), n), nz, ny)
        return pl.ds(pl.multiple_of(f * wide + h * piece, 128), piece)

    def steps_before(q):
        if by_columns:
            k = (q - 2) // 2
            return [(k, (q % 2,))] if 0 < k else []
        ks = [n - 2] if q == n - 1 else [q] if 0 < q < n - 2 else []
        return [(k, (0, 1)) for k in ks]

    def product(q, b):
        made = jnp.dot(
            hidden[rows(b), :], down_full[:, piece_columns(q)], preferred_element_type=f32
        )
        return made.astype(bf16)

    def make(q, dx):
        gone(dx, q)[...] = product(q, x_at(dx) + 1 - 2 * core)
        keep[dx, q] = product(q, x_at(dx))
        pc_copy(dx, q).start()

    def make_far(q):
        for dx in range(1, nx):
            make(q, dx)

    def pair_far(q):
        for dx in range(1, nx):
            pc_copy(dx, q).wait_recv()
            both = keep[dx, q].astype(f32) + got_core[dx, q].astype(f32)
            keep[dx, q] = both.astype(bf16)
            px_copy(dx, q).start()

    def finish(q):
        cols = piece_columns(q)
        pc_copy(0, q).wait_recv()
        total = stream[:, cols].astype(f32) + keep[0, q].astype(f32)
        total = total + got_core[0, q].astype(f32)
        for dx in range(1, nx):
            px_copy(dx, q).wait_recv()
            total = total + got_x[dx - 1, q].astype(f32)
        held[:, cols] = total.astype(bf16)

    def down_step(q, _):
        for at in range(n_piece - 2):
            for k, ways in steps_before(at):

                @pl.when(q == at)
                def _():
                    w_step(2, k, ways)

        make_far(q)
        make(q, 0)
        pair_far(q)

        @pl.when(q > 1)
        def _():
            finish(q - 2)

        return 0

    lax.fori_loop(0, n_piece - 2, down_step, 0)
    last = (n_piece - 2, n_piece - 1)
    for q in last:
        for k, ways in steps_before(q):
            w_step(2, k, ways)
        make_far(q)
    for q in last:
        pair_far(q)
        make(q, 0)
    for q in range(n_piece - 4, n_piece):
        finish(q)
    sent(mix_full.at[pl.ds(0, nx * tok), :], p_send.at[0])
    for dx in range(1, nx):
        sent(mix_full.at[pl.ds(0, tok), :], p_send.at[1])
    w_drain(2)


def make_body(n_fs, n_tp, ny):
    nz, nx = n_fs // ny, n_tp // 2

    def body(
        mixed,
        residual,
        mix_weight,
        norm_gain,
        up_weight,
        gate_weight,
        conv_weight,
        conv_bias,
        down_weight,
    ):
        tok, width = residual.shape
        depth, (hid, wide) = mixed.shape[1], down_weight.shape
        piece = wide // 2 if wide % 256 == 0 else wide
        n_piece = width // piece
        dma = pltpu.SemaphoreType.DMA
        whole = pl.BlockSpec(memory_space=pl.ANY)
        small = pl.BlockSpec(memory_space=pltpu.VMEM)
        held = depth + 3 * hid + n_tp * tok + (3 * nx + 2) * tok
        lanes = (hid + 127) // 128 * 128
        held = held * width * 2 + n_tp * tok * lanes * 8 + (1 << 20)
        split = held <= VMEM
        return pl.pallas_call(
            functools.partial(layer_kernel, nz, ny, nx, split),
            out_shape=pltpu.VMEM((tok, width), bf16),
            in_specs=[whole] * 9,
            out_specs=small,
            scratch_shapes=[
                pltpu.VMEM((1, width), f32),
                pltpu.VMEM((3, hid), f32),
                pltpu.VMEM((hid,), f32),
                pltpu.VMEM((depth, width), bf16),
                pltpu.VMEM((hid, width), bf16),
                pltpu.VMEM((hid, width), bf16),
                pltpu.VMEM((hid, width), bf16),
                pltpu.VMEM((n_tp * tok, width), bf16),
                pltpu.VMEM((n_tp * tok + 16, hid), bf16),
                pltpu.VMEM((n_tp * tok, hid), bf16),
                pltpu.VMEM((n_tp * tok, hid) if split else (8, 128), f32),
                pltpu.VMEM((tok, depth), bf16),
                pltpu.VMEM((tok, width), bf16),
                pltpu.VMEM((nx, n_piece, tok, piece), bf16),
                pltpu.VMEM((nx, n_piece, tok, piece), bf16),
                pltpu.VMEM((max(nx - 1, 1), n_piece, tok, piece), bf16),
                dma((3,)),
                dma((3, n_fs, 2)),
                dma((3,)),
                dma((n_fs, 2)),
                dma((n_fs, max(nx - 1, 1))),
                dma((1,)),
                dma((2,)),
                dma((n_tp,)),
                dma((2,)),
                dma((n_piece, nx)),
                dma((n_piece, max(nx - 1, 1))),
                dma((9,)),
            ],
            compiler_params=pltpu.CompilerParams(
                collective_id=0, has_side_effects=True, vmem_limit_bytes=VMEM - 2 * tok * width * 2
            ),
        )(
            mixed,
            residual,
            mix_weight,
            up_weight.T,
            gate_weight.T,
            down_weight,
            norm_gain[None, :],
            conv_weight,
            conv_bias,
        )

    return body


def solution(mesh):
    coords = [getattr(d, "coords", None) for d in mesh.devices[:, 0]]
    n_fs, n_tp = mesh.shape["fs"], mesh.shape["tp"]
    ny = len({c[1] for c in coords}) if None not in coords else 1
    if n_fs % ny:
        ny = 1
    return jax.shard_map(
        make_body(n_fs, n_tp, ny),
        mesh=mesh,
        in_specs=(
            P(("fs", "tp"), None),
            P(("fs", "tp"), None),
            P(("fs", "tp"), None),
            P(),
            P("fs", "tp"),
            P("fs", "tp"),
            P(None, "tp"),
            P("tp"),
            P("tp", "fs"),
        ),
        out_specs=P(("fs", "tp"), None),
        check_vma=False,
    )
```

```python
import functools

import jax
import jax.numpy as jnp
from jax import lax
from jax.experimental import pallas as pl
from jax.experimental.pallas import tpu as pltpu
from jax.sharding import PartitionSpec as P

norm_eps = 1e-06
f32, bf16 = jnp.float32, jnp.bfloat16
MESH = pl.DeviceIdType.MESH
NT = (((1,), (1,)), ((), ()))
TILE = 256
VMEM = 67043328


def mod(a, n):
    return lax.rem(a + n, n)


def ring_place(f, nz, ny):
    z, y = lax.div(f, ny), lax.rem(f, ny)
    if ny == 1:
        return z
    along = jnp.where(lax.rem(z, 2) == 0, y - 1, ny - 1 - y)
    return jnp.where(y == 0, nz * (ny - 1) + nz - 1 - z, z * (ny - 1) + along)


def ring_chip(r, nz, ny):
    if ny == 1:
        return r
    z, k = lax.div(r, ny - 1), lax.rem(r, ny - 1)
    out = z * ny + jnp.where(lax.rem(z, 2) == 0, 1 + k, ny - 1 - k)
    return jnp.where(r < nz * (ny - 1), out, (nz - 1 - (r - nz * (ny - 1))) * ny)


def layer_kernel(
    nz,
    ny,
    nx,
    split,
    mixed,
    residual,
    mix_shard,
    up_shard,
    gate_shard,
    down_shard,
    gain_in,
    taps_in,
    bias_in,
    held,
    gain,
    taps,
    bias,
    mix_full,
    up_full,
    gate_full,
    down_full,
    tokens,
    up_part,
    hidden,
    gate_sum,
    mixed_v,
    stream,
    keep,
    got_core,
    got_x,
    w_send,
    w_recv,
    m_send,
    m_recv,
    m_core_recv,
    t_send,
    t_recv,
    p_send,
    pc_recv,
    px_recv,
    in_sem,
):
    n = nz * ny
    half_n = n // 2
    n_tp = 2 * nx
    me = lax.axis_index("fs")
    tp = lax.axis_index("tp")
    x, core = lax.div(tp, 2), lax.rem(tp, 2)
    place = ring_place(me, nz, ny)

    chips = [ring_chip(mod(place + d, n), nz, ny) for d in range(n)]

    def ring(d):
        return chips[d % n]

    nxt, prv = ring(1), ring(-1)
    twin = tp + 1 - 2 * core

    def x_at(dx):
        return lax.rem(x + dx, nx) * 2 + core

    tok, width = stream.shape
    hid, wide = up_shard.shape
    by_columns = wide % 256 == 0
    cut = wide // 2 if by_columns else (hid // 2 + 15) // 16 * 16
    halves = ((0, cut), (cut, (wide if by_columns else hid) - cut))
    fulls = (up_full, gate_full, down_full)
    shards = (up_shard, gate_shard, down_shard)
    n_step = n - 3
    mrows = mix_shard.shape[0]
    front = width // 2
    mix_cut = ((0, front), (front, width - front))
    n_piece, piece = keep.shape[1], keep.shape[3]

    def remote(src, dst, send, recv, axis, to):
        return pltpu.make_async_remote_copy(
            src_ref=src,
            dst_ref=dst,
            send_sem=send,
            recv_sem=recv,
            device_id={axis: to},
            device_id_type=MESH,
        )

    def columns(f):
        return pl.ds(pl.multiple_of(f * wide, 128), wide)

    def slot(m, f, h):
        off, size = halves[h]
        if by_columns:
            return fulls[m].at[:, pl.ds(pl.multiple_of(f * wide + off, 128), size)]
        return fulls[m].at[pl.ds(off, size), columns(f)]

    def w_copy(m, f, h, way, mine=False):
        at = pl.ds(*halves[h])
        src = slot(m, f, h)
        if mine:
            src = shards[m].at[:, at] if by_columns else shards[m].at[at, :]
        to = prv if way else nxt
        return remote(src, slot(m, f, h), w_send.at[m], w_recv.at[m % 2, f, h], "fs", to)

    def w_own(m):
        for k in range(2):
            w_copy(m, me, k, 0, True).start()
            w_copy(m, me, 1 - k, 1, True).start()

    def w_step(m, k, ways=(0, 1)):
        d = 1 + k // 2
        for way in ways:
            f, hh = (ring(d), 1 - k % 2) if way else (ring(-d), k % 2)
            w_copy(m, f, hh, way).wait_recv()
            if k < n_step:
                w_copy(m, f, hh, way).start()

    def sent(ref, sem):
        remote(ref, ref, sem, sem, "fs", nxt).wait_send()

    def w_drain(m):
        sent(fulls[m].at[:, pl.ds(0, (n - 1) * wide)], w_send.at[m])

    def w_local(m):
        return pltpu.make_async_copy(shards[m], fulls[m].at[:, columns(me)], in_sem.at[m])

    def part(f, t):
        return mix_full.at[pl.ds(pl.multiple_of((f * n_tp + t) * mrows, 16), mrows), :]

    def m_half(f, h):
        return part(f, tp).at[:, pl.ds(*mix_cut[h])]

    def m_ring(f, h, way, mine=False):
        src = m_half(f, h)
        if mine:
            src = mix_shard.at[:, pl.ds(*mix_cut[h])]
        to = prv if way else nxt
        return remote(src, m_half(f, h), m_send.at[0], w_recv.at[1, f, h], "fs", to)

    def m_x(f, dx, mine=False):
        src = mix_shard if mine else part(f, tp)
        return remote(src, part(f, tp), m_send.at[1], m_recv.at[f, dx - 1], "tp", x_at(dx))

    def m_core(f, dx, mine=False):
        t = x_at(dx)
        src = mix_shard if mine else part(f, t)
        return remote(src, part(f, t), m_send.at[2], m_core_recv.at[0], "tp", twin)

    def m_spread(f, mine=False):
        for dx in range(1, nx):
            m_x(f, dx, mine).start()
        m_core(f, 0, mine).start()

    def m_wait(f, t, got):
        remote(part(f, t), part(f, t), m_send.at[2], got, "tp", twin).wait_recv()

    def m_own():
        for k in range(2):
            m_ring(me, k, 0, True).start()
            m_ring(me, 1 - k, 1, True).start()

    def m_step(d):
        for k in (2 * d - 2, 2 * d - 1):
            for way, f, h in ((0, ring(-d), k % 2), (1, ring(d), 1 - k % 2)):
                if k < n - 1:
                    m_ring(f, h, way).wait_recv()
                if k < n_step:
                    m_ring(f, h, way).start()
        for f in (ring(-d), ring(d)) if d < half_n else (ring(d),):
            m_spread(f)

    def m_relay(f):
        for dx in range(1, nx):
            m_wait(f, x_at(dx), m_recv.at[f, nx - dx - 1])
            m_core(f, dx).start()

    def m_drain():
        for lane, count in enumerate((n - 1, n * (nx - 1), n * nx)):
            sent(mix_full.at[pl.ds(0, count * mrows), :], m_send.at[lane])

    def rows(b):
        return pl.ds(pl.multiple_of(b * tok, 16), tok)

    def t_copy(b, send, to):
        return remote(tokens.at[rows(b), :], tokens.at[rows(b), :], send, t_recv.at[b], "tp", to)

    def t_wait(b):
        t_copy(b, t_send.at[1], twin).wait_recv()

    def gone(dx, q):
        at = pl.multiple_of(q * piece, 128)
        return mix_full.at[pl.ds(dx * tok, tok), pl.ds(at, piece)]

    def pc_copy(dx, q):
        return remote(
            gone(dx, q), got_core.at[dx, q], p_send.at[0], pc_recv.at[q, dx], "tp", twin
        )

    def px_copy(dx, q):
        src, dst = keep.at[dx, q], got_x.at[dx - 1, q]
        return remote(src, dst, p_send.at[1], px_recv.at[q, dx - 1], "tp", x_at(dx))

    load_mixed = pltpu.make_async_copy(mixed, mixed_v, in_sem.at[3])
    load_residual = pltpu.make_async_copy(residual, held, in_sem.at[4])
    load_mix = pltpu.make_async_copy(mix_shard, part(me, tp), in_sem.at[5])
    small_loads = [
        pltpu.make_async_copy(src, dst, in_sem.at[6 + i])
        for i, (src, dst) in enumerate(((gain_in, gain), (taps_in, taps), (bias_in, bias)))
    ]

    barrier = pltpu.get_barrier_semaphore()
    for other in (nxt, prv):
        pl.semaphore_signal(barrier, inc=1, device_id={"fs": other}, device_id_type=MESH)
    for other in [twin] + [x_at(dx) for dx in range(1, nx)]:
        pl.semaphore_signal(barrier, inc=1, device_id={"tp": other}, device_id_type=MESH)
    pl.semaphore_wait(barrier, 2 + nx)

    m_own()
    m_spread(me, True)
    load_mix.start()
    load_mixed.start()
    load_residual.start()
    for load in small_loads:
        load.start()
    for m in range(3):
        w_local(m).start()
    up_part[0:16, :] = jnp.zeros((16, hid), bf16)

    early = min(n_step, half_n - 1)
    for d in range(1, half_n + 1):
        m_step(d)
        if d == 1:
            w_own(0)
        if 2 <= d < early + 2:
            w_step(0, d - 2)
    for q in range(n):
        d = (q + 1) // 2
        m_relay(ring(-d if q % 2 else d))
    from_twin = mix_full.at[pl.ds(0, n * nx * mrows), :]
    remote(from_twin, from_twin, m_send.at[2], m_core_recv.at[0], "tp", twin).wait_recv()
    load_mix.wait()
    load_mixed.wait()
    load_residual.wait()
    for load in small_loads:
        load.wait()

    def project(i, _):
        cols = pl.ds(pl.multiple_of(i * TILE, 128), TILE)
        made = jnp.dot(mixed_v[...], mix_full[:, cols], preferred_element_type=f32)
        stream[:, cols] = (held[:, cols].astype(f32) + made).astype(bf16)
        return 0

    lax.fori_loop(0, width // TILE, project, 0)

    for k in range(early, min(early + 1, n_step)):
        w_step(0, k)

    def norm(i, _):
        at = pl.multiple_of(i * 32, 16)
        row = stream[pl.ds(at, 32), :].astype(f32)
        scale = lax.rsqrt(jnp.mean(row * row, axis=-1, keepdims=True) + norm_eps)
        tokens[pl.ds(pl.multiple_of(tp * tok + at, 16), 32), :] = (row * scale * gain[...]).astype(
            bf16
        )
        return 0

    lax.fori_loop(0, tok // 32, norm, 0)
    for dx in range(1, nx):
        t_copy(tp, t_send.at[0], x_at(dx)).start()
    t_copy(tp, t_send.at[1], twin).start()

    for k in range(min(early + 1, n_step), n_step):
        w_step(0, k)
    w_own(1)
    for k in range(n_step, n - 1):
        w_step(0, k)
    w_local(0).wait()

    def block_of(j):
        return lax.rem(x + lax.div(j, 2), nx) * 2 + lax.rem(core + lax.rem(j, 2), 2)

    def up_block(j, _):
        b = block_of(j)

        @pl.when(j > 0)
        def _():
            t_wait(b)

        @pl.when((j > 1) & (lax.rem(j, 2) == 0))
        def _():
            t_copy(b, t_send.at[1], twin).start()

        for lo in range(0, hid, TILE):
            hi = min(lo + TILE, hid)
            made = lax.dot_general(
                tokens[rows(b), :], up_full[lo:hi, :], NT, preferred_element_type=f32
            )
            up_part[pl.ds(pl.multiple_of(16 + b * tok, 16), tok), lo:hi] = made.astype(bf16)
        for at, ks in ((1, (0, 1)), (n_tp - 2, (2,))):
            for k in ks:
                if k < ahead:

                    @pl.when(j == at)
                    def _():
                        w_step(1, k)

        return 0

    ahead = min(3, n_step)
    lax.fori_loop(0, n_tp, up_block, 0)

    def gate_dot(b, lo, hi, fs):
        made = None
        for f in fs:
            term = lax.dot_general(
                tokens[rows(b), columns(f)],
                gate_full[lo:hi, columns(f)],
                NT,
                preferred_element_type=f32,
            )
            made = term if made is None else made + term
        return made

    def gate_pass(d):
        fs = ([me] if d == 1 else []) + [ring(-d), ring(d)]

        def add(b, _):
            for lo in range(0, hid, TILE):
                hi = min(lo + TILE, hid)
                made = gate_dot(b, lo, hi, fs)
                if d > 1:
                    made = gate_sum[rows(b), lo:hi] + made
                gate_sum[rows(b), lo:hi] = made
            return 0

        lax.fori_loop(0, n_tp, add, 0)

    w_local(1).wait()
    for d in range(1, half_n):
        for k in (2 * d - 2, 2 * d - 1):
            if k >= ahead:
                w_step(1, k)
            if k == n_step - 1:
                w_own(2)
        if split:
            gate_pass(d)
    w_step(1, n - 2)
    m_drain()
    for lane in range(2):
        sent(tokens.at[pl.ds(0, (nx - 1 + lane) * tok), :], t_send.at[lane])
    for m in range(2):
        w_drain(m)

    def gate_block(j, _):
        b = block_of(j)
        for lo in range(0, hid, TILE):
            hi = min(lo + TILE, hid)
            if split:
                made = gate_sum[rows(b), lo:hi] + gate_dot(b, lo, hi, [ring(half_n)])
            else:
                made = lax.dot_general(
                    tokens[rows(b), :], gate_full[lo:hi, :], NT, preferred_element_type=f32
                )
            gated = made.astype(bf16).astype(f32)
            window = up_part[pl.ds(pl.multiple_of(b * tok, 16), tok + 16), lo:hi].astype(f32)
            smoothed = bias[lo:hi][None, :]
            for k in range(3):
                moved = window if k == 2 else pltpu.roll(window, 2 - k, 0)
                smoothed = smoothed + taps[k : k + 1, lo:hi] * moved[16:, :]
            hidden[rows(b), lo:hi] = (jax.nn.gelu(smoothed) * gated).astype(bf16)

        @pl.when(j == n_tp - 2)
        def _():
            w_step(2, 0)

        return 0

    lax.fori_loop(0, n_tp, gate_block, 0)
    w_local(2).wait()

    def piece_columns(q):
        if by_columns:
            k, way = lax.div(jnp.maximum(q - 2, 0), 2), lax.rem(q, 2)
            d = jnp.where(q < 2, 0, 1 + lax.div(k, 2))
            h = jnp.where(way == 0, lax.rem(k, 2), 1 - lax.rem(k, 2))
        else:
            d, h, way = lax.div(q + 1, 2), 0, 1 - lax.rem(q, 2)
        f = ring_chip(mod(place + jnp.where(way == 0, -d, d), n), nz, ny)
        return pl.ds(pl.multiple_of(f * wide + h * piece, 128), piece)

    def steps_before(q):
        if by_columns:
            k = (q - 2) // 2
            return [(k, (q % 2,))] if 0 < k else []
        ks = [n - 2] if q == n - 1 else [q] if 0 < q < n - 2 else []
        return [(k, (0, 1)) for k in ks]

    def product(q, b):
        made = jnp.dot(
            hidden[rows(b), :], down_full[:, piece_columns(q)], preferred_element_type=f32
        )
        return made.astype(bf16)

    def make(q, dx):
        gone(dx, q)[...] = product(q, x_at(dx) + 1 - 2 * core)
        keep[dx, q] = product(q, x_at(dx))
        pc_copy(dx, q).start()

    def make_far(q):
        for dx in range(1, nx):
            make(q, dx)

    def pair_far(q):
        for dx in range(1, nx):
            pc_copy(dx, q).wait_recv()
            both = keep[dx, q].astype(f32) + got_core[dx, q].astype(f32)
            keep[dx, q] = both.astype(bf16)
            px_copy(dx, q).start()

    def finish(q):
        cols = piece_columns(q)
        pc_copy(0, q).wait_recv()
        total = stream[:, cols].astype(f32) + keep[0, q].astype(f32)
        total = total + got_core[0, q].astype(f32)
        for dx in range(1, nx):
            px_copy(dx, q).wait_recv()
            total = total + got_x[dx - 1, q].astype(f32)
        held[:, cols] = total.astype(bf16)

    def down_step(q, _):
        for at in range(n_piece - 2):
            for k, ways in steps_before(at):

                @pl.when(q == at)
                def _():
                    w_step(2, k, ways)

        make_far(q)
        make(q, 0)
        pair_far(q)

        @pl.when(q > 1)
        def _():
            finish(q - 2)

        return 0

    lax.fori_loop(0, n_piece - 2, down_step, 0)
    last = (n_piece - 2, n_piece - 1)
    for q in last:
        for k, ways in steps_before(q):
            w_step(2, k, ways)
        make_far(q)
    for q in last:
        pair_far(q)
        make(q, 0)
    for q in range(n_piece - 4, n_piece):
        finish(q)
    sent(mix_full.at[pl.ds(0, nx * tok), :], p_send.at[0])
    for dx in range(1, nx):
        sent(mix_full.at[pl.ds(0, tok), :], p_send.at[1])
    w_drain(2)


def make_body(n_fs, n_tp, ny):
    nz, nx = n_fs // ny, n_tp // 2

    def body(
        mixed,
        residual,
        mix_weight,
        norm_gain,
        up_weight,
        gate_weight,
        conv_weight,
        conv_bias,
        down_weight,
    ):
        tok, width = residual.shape
        depth, (hid, wide) = mixed.shape[1], down_weight.shape
        piece = wide // 2 if wide % 256 == 0 else wide
        n_piece = width // piece
        dma = pltpu.SemaphoreType.DMA
        whole = pl.BlockSpec(memory_space=pl.ANY)
        small = pl.BlockSpec(memory_space=pltpu.VMEM)
        held = depth + 3 * hid + n_tp * tok + (3 * nx + 2) * tok
        lanes = (hid + 127) // 128 * 128
        held = held * width * 2 + n_tp * tok * lanes * 8 + (1 << 20)
        split = held <= VMEM
        return pl.pallas_call(
            functools.partial(layer_kernel, nz, ny, nx, split),
            out_shape=pltpu.VMEM((tok, width), bf16),
            in_specs=[whole] * 9,
            out_specs=small,
            scratch_shapes=[
                pltpu.VMEM((1, width), f32),
                pltpu.VMEM((3, hid), f32),
                pltpu.VMEM((hid,), f32),
                pltpu.VMEM((depth, width), bf16),
                pltpu.VMEM((hid, width), bf16),
                pltpu.VMEM((hid, width), bf16),
                pltpu.VMEM((hid, width), bf16),
                pltpu.VMEM((n_tp * tok, width), bf16),
                pltpu.VMEM((n_tp * tok + 16, hid), bf16),
                pltpu.VMEM((n_tp * tok, hid), bf16),
                pltpu.VMEM((n_tp * tok, hid) if split else (8, 128), f32),
                pltpu.VMEM((tok, depth), bf16),
                pltpu.VMEM((tok, width), bf16),
                pltpu.VMEM((nx, n_piece, tok, piece), bf16),
                pltpu.VMEM((nx, n_piece, tok, piece), bf16),
                pltpu.VMEM((max(nx - 1, 1), n_piece, tok, piece), bf16),
                dma((3,)),
                dma((2, n_fs, 2)),
                dma((3,)),
                dma((n_fs, max(nx - 1, 1))),
                dma((1,)),
                dma((2,)),
                dma((n_tp,)),
                dma((2,)),
                dma((n_piece, nx)),
                dma((n_piece, max(nx - 1, 1))),
                dma((9,)),
            ],
            compiler_params=pltpu.CompilerParams(
                collective_id=0, has_side_effects=True, vmem_limit_bytes=VMEM - 2 * tok * width * 2
            ),
        )(
            mixed,
            residual,
            mix_weight,
            up_weight.T,
            gate_weight.T,
            down_weight,
            norm_gain[None, :],
            conv_weight,
            conv_bias,
        )

    return body


def solution(mesh):
    coords = [getattr(d, "coords", None) for d in mesh.devices[:, 0]]
    n_fs, n_tp = mesh.shape["fs"], mesh.shape["tp"]
    ny = len({c[1] for c in coords}) if None not in coords else 1
    if n_fs % ny:
        ny = 1
    return jax.shard_map(
        make_body(n_fs, n_tp, ny),
        mesh=mesh,
        in_specs=(
            P(("fs", "tp"), None),
            P(("fs", "tp"), None),
            P(("fs", "tp"), None),
            P(),
            P("fs", "tp"),
            P("fs", "tp"),
            P(None, "tp"),
            P("tp"),
            P("tp", "fs"),
        ),
        out_specs=P(("fs", "tp"), None),
        check_vma=False,
    )
```

```python
import functools

import jax
import jax.numpy as jnp
from jax import lax
from jax.experimental import pallas as pl
from jax.experimental.pallas import tpu as pltpu
from jax.sharding import PartitionSpec as P

norm_eps = 1e-06
f32, bf16 = jnp.float32, jnp.bfloat16
MESH = pl.DeviceIdType.MESH
NT = (((1,), (1,)), ((), ()))
TILE = 256
VMEM = 67043328


def mod(a, n):
    return lax.rem(a + n, n)


def ring_place(f, nz, ny):
    z, y = lax.div(f, ny), lax.rem(f, ny)
    if ny == 1:
        return z
    along = jnp.where(lax.rem(z, 2) == 0, y - 1, ny - 1 - y)
    return jnp.where(y == 0, nz * (ny - 1) + nz - 1 - z, z * (ny - 1) + along)


def ring_chip(r, nz, ny):
    if ny == 1:
        return r
    z, k = lax.div(r, ny - 1), lax.rem(r, ny - 1)
    out = z * ny + jnp.where(lax.rem(z, 2) == 0, 1 + k, ny - 1 - k)
    return jnp.where(r < nz * (ny - 1), out, (nz - 1 - (r - nz * (ny - 1))) * ny)


def layer_kernel(
    nz,
    ny,
    nx,
    split,
    mixed,
    residual,
    mix_shard,
    up_shard,
    gate_shard,
    down_shard,
    gain_in,
    taps_in,
    bias_in,
    held,
    gain,
    taps,
    bias,
    mix_full,
    up_full,
    gate_full,
    down_full,
    tokens,
    up_part,
    hidden,
    gate_sum,
    mixed_v,
    stream,
    keep,
    got_core,
    got_x,
    w_send,
    w_recv,
    m_send,
    m_recv,
    m_core_recv,
    t_send,
    t_recv,
    p_send,
    pc_recv,
    near_recv,
    px_recv,
    in_sem,
):
    n = nz * ny
    half_n = n // 2
    n_tp = 2 * nx
    me = lax.axis_index("fs")
    tp = lax.axis_index("tp")
    x, core = lax.div(tp, 2), lax.rem(tp, 2)
    place = ring_place(me, nz, ny)

    chips = [ring_chip(mod(place + d, n), nz, ny) for d in range(n)]

    def ring(d):
        return chips[d % n]

    nxt, prv = ring(1), ring(-1)
    twin = tp + 1 - 2 * core

    def x_at(dx):
        return lax.rem(x + dx, nx) * 2 + core

    tok, width = stream.shape
    hid, wide = up_shard.shape
    by_columns = wide % 256 == 0
    cut = wide // 2 if by_columns else (hid // 2 + 15) // 16 * 16
    halves = ((0, cut), (cut, (wide if by_columns else hid) - cut))
    fulls = (up_full, gate_full, down_full)
    shards = (up_shard, gate_shard, down_shard)
    n_step = n - 3
    mrows = mix_shard.shape[0]
    front = width // 2
    mix_cut = ((0, front), (front, width - front))
    n_piece, piece = keep.shape[1], keep.shape[3]

    def remote(src, dst, send, recv, axis, to):
        return pltpu.make_async_remote_copy(
            src_ref=src,
            dst_ref=dst,
            send_sem=send,
            recv_sem=recv,
            device_id={axis: to},
            device_id_type=MESH,
        )

    def columns(f):
        return pl.ds(pl.multiple_of(f * wide, 128), wide)

    def slot(m, f, h):
        off, size = halves[h]
        if by_columns:
            return fulls[m].at[:, pl.ds(pl.multiple_of(f * wide + off, 128), size)]
        return fulls[m].at[pl.ds(off, size), columns(f)]

    def w_copy(m, f, h, way, mine=False):
        at = pl.ds(*halves[h])
        src = slot(m, f, h)
        if mine:
            src = shards[m].at[:, at] if by_columns else shards[m].at[at, :]
        to = prv if way else nxt
        return remote(src, slot(m, f, h), w_send.at[m], w_recv.at[m % 2, f, h], "fs", to)

    def w_own(m):
        for k in range(2):
            w_copy(m, me, k, 0, True).start()
            w_copy(m, me, 1 - k, 1, True).start()

    def w_step(m, k, ways=(0, 1)):
        d = 1 + k // 2
        for way in ways:
            f, hh = (ring(d), 1 - k % 2) if way else (ring(-d), k % 2)
            w_copy(m, f, hh, way).wait_recv()
            if k < n_step:
                w_copy(m, f, hh, way).start()

    def sent(ref, sem):
        remote(ref, ref, sem, sem, "fs", nxt).wait_send()

    def w_drain(m):
        sent(fulls[m].at[:, pl.ds(0, (n - 1) * wide)], w_send.at[m])

    def w_local(m):
        return pltpu.make_async_copy(shards[m], fulls[m].at[:, columns(me)], in_sem.at[m])

    def part(f, t):
        return mix_full.at[pl.ds(pl.multiple_of((f * n_tp + t) * mrows, 16), mrows), :]

    def m_half(f, h):
        return part(f, tp).at[:, pl.ds(*mix_cut[h])]

    def m_ring(f, h, way, mine=False):
        src = m_half(f, h)
        if mine:
            src = mix_shard.at[:, pl.ds(*mix_cut[h])]
        to = prv if way else nxt
        return remote(src, m_half(f, h), m_send.at[0], w_recv.at[1, f, h], "fs", to)

    def m_x(f, dx, mine=False):
        src = mix_shard if mine else part(f, tp)
        return remote(src, part(f, tp), m_send.at[1], m_recv.at[f, dx - 1], "tp", x_at(dx))

    def m_core(f, dx, mine=False):
        t = x_at(dx)
        src = mix_shard if mine else part(f, t)
        return remote(src, part(f, t), m_send.at[2], m_core_recv.at[0], "tp", twin)

    def m_spread(f, mine=False):
        for dx in range(1, nx):
            m_x(f, dx, mine).start()
        m_core(f, 0, mine).start()

    def m_wait(f, t, got):
        remote(part(f, t), part(f, t), m_send.at[2], got, "tp", twin).wait_recv()

    def m_own():
        for k in range(2):
            m_ring(me, k, 0, True).start()
            m_ring(me, 1 - k, 1, True).start()

    def m_step(d):
        for k in (2 * d - 2, 2 * d - 1):
            for way, f, h in ((0, ring(-d), k % 2), (1, ring(d), 1 - k % 2)):
                if k < n - 1:
                    m_ring(f, h, way).wait_recv()
                if k < n_step:
                    m_ring(f, h, way).start()
        for f in (ring(-d), ring(d)) if d < half_n else (ring(d),):
            m_spread(f)

    def m_relay(f):
        for dx in range(1, nx):
            m_wait(f, x_at(dx), m_recv.at[f, nx - dx - 1])
            m_core(f, dx).start()

    def m_drain():
        for lane, count in enumerate((n - 1, n * (nx - 1), n * nx)):
            sent(mix_full.at[pl.ds(0, count * mrows), :], m_send.at[lane])

    def rows(b):
        return pl.ds(pl.multiple_of(b * tok, 16), tok)

    def t_copy(b, send, to):
        return remote(tokens.at[rows(b), :], tokens.at[rows(b), :], send, t_recv.at[b], "tp", to)

    def t_wait(b):
        t_copy(b, t_send.at[1], twin).wait_recv()

    def gone(dx, q):
        at = pl.multiple_of(q * piece, 128)
        return mix_full.at[pl.ds(dx * tok, tok), pl.ds(at, piece)]

    def pair_at(q):
        if isinstance(q, int):
            return q // 2 + (1 if q == n_piece - 1 else 0)
        return lax.div(q, 2)

    def pc_copy(dx, q):
        got = pc_recv.at[q, dx - 1] if dx else near_recv.at[pair_at(q)]
        return remote(gone(dx, q), got_core.at[dx, q], p_send.at[0], got, "tp", twin)

    def px_copy(dx, q):
        src, dst = keep.at[dx, q], got_x.at[dx - 1, q]
        return remote(src, dst, p_send.at[1], px_recv.at[pair_at(q), dx - 1], "tp", x_at(dx))

    def wait_pieces(ref, got):
        remote(ref, ref, p_send.at[0], got, "tp", twin).wait_recv()

    load_mixed = pltpu.make_async_copy(mixed, mixed_v, in_sem.at[3])
    load_residual = pltpu.make_async_copy(residual, held, in_sem.at[4])
    load_mix = pltpu.make_async_copy(mix_shard, part(me, tp), in_sem.at[5])
    small_loads = [
        pltpu.make_async_copy(src, dst, in_sem.at[6 + i])
        for i, (src, dst) in enumerate(((gain_in, gain), (taps_in, taps), (bias_in, bias)))
    ]

    barrier = pltpu.get_barrier_semaphore()
    for other in (nxt, prv):
        pl.semaphore_signal(barrier, inc=1, device_id={"fs": other}, device_id_type=MESH)
    for other in [twin] + [x_at(dx) for dx in range(1, nx)]:
        pl.semaphore_signal(barrier, inc=1, device_id={"tp": other}, device_id_type=MESH)
    pl.semaphore_wait(barrier, 2 + nx)

    m_own()
    m_spread(me, True)
    load_mix.start()
    load_mixed.start()
    load_residual.start()
    for load in small_loads:
        load.start()
    for m in range(3):
        w_local(m).start()
    up_part[0:16, :] = jnp.zeros((16, hid), bf16)

    early = min(n_step, half_n - 1)
    for d in range(1, half_n + 1):
        m_step(d)
        if d == 1:
            w_own(0)
        if 2 <= d < early + 2:
            w_step(0, d - 2)
    for q in range(n):
        d = (q + 1) // 2
        m_relay(ring(-d if q % 2 else d))
    from_twin = mix_full.at[pl.ds(0, n * nx * mrows), :]
    remote(from_twin, from_twin, m_send.at[2], m_core_recv.at[0], "tp", twin).wait_recv()
    load_mix.wait()
    load_mixed.wait()
    load_residual.wait()
    for load in small_loads:
        load.wait()

    def project(i, _):
        cols = pl.ds(pl.multiple_of(i * TILE, 128), TILE)
        made = jnp.dot(mixed_v[...], mix_full[:, cols], preferred_element_type=f32)
        stream[:, cols] = (held[:, cols].astype(f32) + made).astype(bf16)
        return 0

    lax.fori_loop(0, width // TILE, project, 0)

    for k in range(early, min(early + 1, n_step)):
        w_step(0, k)

    def norm(i, _):
        at = pl.multiple_of(i * 32, 16)
        row = stream[pl.ds(at, 32), :].astype(f32)
        scale = lax.rsqrt(jnp.mean(row * row, axis=-1, keepdims=True) + norm_eps)
        tokens[pl.ds(pl.multiple_of(tp * tok + at, 16), 32), :] = (row * scale * gain[...]).astype(
            bf16
        )
        return 0

    lax.fori_loop(0, tok // 32, norm, 0)
    for dx in range(1, nx):
        t_copy(tp, t_send.at[0], x_at(dx)).start()
    t_copy(tp, t_send.at[1], twin).start()

    for k in range(min(early + 1, n_step), n_step):
        w_step(0, k)
    w_own(1)
    for k in range(n_step, n - 1):
        w_step(0, k)
    w_local(0).wait()

    def block_of(j):
        return lax.rem(x + lax.div(j, 2), nx) * 2 + lax.rem(core + lax.rem(j, 2), 2)

    def up_block(j, _):
        b = block_of(j)

        @pl.when(j > 0)
        def _():
            t_wait(b)

        @pl.when((j > 1) & (lax.rem(j, 2) == 0))
        def _():
            t_copy(b, t_send.at[1], twin).start()

        for lo in range(0, hid, TILE):
            hi = min(lo + TILE, hid)
            made = lax.dot_general(
                tokens[rows(b), :], up_full[lo:hi, :], NT, preferred_element_type=f32
            )
            up_part[pl.ds(pl.multiple_of(16 + b * tok, 16), tok), lo:hi] = made.astype(bf16)
        for at, ks in ((1, (0, 1)), (n_tp - 2, (2,))):
            for k in ks:
                if k < ahead:

                    @pl.when(j == at)
                    def _():
                        w_step(1, k)

        return 0

    ahead = min(3, n_step)
    lax.fori_loop(0, n_tp, up_block, 0)

    def gate_dot(b, lo, hi, fs):
        made = None
        for f in fs:
            term = lax.dot_general(
                tokens[rows(b), columns(f)],
                gate_full[lo:hi, columns(f)],
                NT,
                preferred_element_type=f32,
            )
            made = term if made is None else made + term
        return made

    def gate_pass(d):
        fs = ([me] if d == 1 else []) + [ring(-d), ring(d)]

        def add(b, _):
            for lo in range(0, hid, TILE):
                hi = min(lo + TILE, hid)
                made = gate_dot(b, lo, hi, fs)
                if d > 1:
                    made = gate_sum[rows(b), lo:hi] + made
                gate_sum[rows(b), lo:hi] = made
            return 0

        lax.fori_loop(0, n_tp, add, 0)

    w_local(1).wait()
    for d in range(1, half_n):
        for k in (2 * d - 2, 2 * d - 1):
            if k >= ahead:
                w_step(1, k)
            if k == n_step - 1:
                w_own(2)
        if split:
            gate_pass(d)
    w_step(1, n - 2)
    m_drain()
    for lane in range(2):
        sent(tokens.at[pl.ds(0, (nx - 1 + lane) * tok), :], t_send.at[lane])
    for m in range(2):
        w_drain(m)

    def gate_block(j, _):
        b = block_of(j)
        for lo in range(0, hid, TILE):
            hi = min(lo + TILE, hid)
            if split:
                made = gate_sum[rows(b), lo:hi] + gate_dot(b, lo, hi, [ring(half_n)])
            else:
                made = lax.dot_general(
                    tokens[rows(b), :], gate_full[lo:hi, :], NT, preferred_element_type=f32
                )
            gated = made.astype(bf16).astype(f32)
            window = up_part[pl.ds(pl.multiple_of(b * tok, 16), tok + 16), lo:hi].astype(f32)
            smoothed = bias[lo:hi][None, :]
            for k in range(3):
                moved = window if k == 2 else pltpu.roll(window, 2 - k, 0)
                smoothed = smoothed + taps[k : k + 1, lo:hi] * moved[16:, :]
            hidden[rows(b), lo:hi] = (jax.nn.gelu(smoothed) * gated).astype(bf16)

        @pl.when(j == n_tp - 2)
        def _():
            w_step(2, 0)

        return 0

    lax.fori_loop(0, n_tp, gate_block, 0)
    w_local(2).wait()

    def piece_columns(q):
        if by_columns:
            k, way = lax.div(jnp.maximum(q - 2, 0), 2), lax.rem(q, 2)
            d = jnp.where(q < 2, 0, 1 + lax.div(k, 2))
            h = jnp.where(way == 0, lax.rem(k, 2), 1 - lax.rem(k, 2))
        else:
            d, h, way = lax.div(q + 1, 2), 0, 1 - lax.rem(q, 2)
        f = ring_chip(mod(place + jnp.where(way == 0, -d, d), n), nz, ny)
        return pl.ds(pl.multiple_of(f * wide + h * piece, 128), piece)

    def steps_before(q):
        if by_columns:
            k = (q - 2) // 2
            return [(k, (q % 2,))] if 0 < k else []
        ks = [n - 2] if q == n - 1 else [q] if 0 < q < n - 2 else []
        return [(k, (0, 1)) for k in ks]

    def product(q, b):
        made = jnp.dot(
            hidden[rows(b), :], down_full[:, piece_columns(q)], preferred_element_type=f32
        )
        return made.astype(bf16)

    def make(q, dx):
        gone(dx, q)[...] = product(q, x_at(dx) + 1 - 2 * core)
        keep[dx, q] = product(q, x_at(dx))
        pc_copy(dx, q).start()

    def make_far(q):
        for dx in range(1, nx):
            make(q, dx)

    def pair_far(q):
        for dx in range(1, nx):
            pc_copy(dx, q).wait_recv()
            both = keep[dx, q].astype(f32) + got_core[dx, q].astype(f32)
            keep[dx, q] = both.astype(bf16)
            px_copy(dx, q).start()

    def finish(q, count):
        wait_pieces(got_core.at[0, pl.ds(q, count)], near_recv.at[pair_at(q)])
        for dx in range(1, nx):
            wait_pieces(got_x.at[dx - 1, pl.ds(q, count)], px_recv.at[pair_at(q), dx - 1])
        for i in range(count):
            cols = piece_columns(q + i)
            total = stream[:, cols].astype(f32) + keep[0, q + i].astype(f32)
            total = total + got_core[0, q + i].astype(f32)
            for dx in range(1, nx):
                total = total + got_x[dx - 1, q + i].astype(f32)
            held[:, cols] = total.astype(bf16)

    def down_step(q, _):
        for at in range(n_piece - 2):
            for k, ways in steps_before(at):

                @pl.when(q == at)
                def _():
                    w_step(2, k, ways)

        make_far(q)
        make(q, 0)
        pair_far(q)

        @pl.when((q > 2) & (lax.rem(q, 2) == 1))
        def _():
            finish(q - 3, 2)

        return 0

    lax.fori_loop(0, n_piece - 2, down_step, 0)
    last = (n_piece - 2, n_piece - 1)
    for q in last:
        for k, ways in steps_before(q):
            w_step(2, k, ways)
        make_far(q)
    for q in last:
        pair_far(q)
        make(q, 0)
    finish(n_piece - 4, 2)
    for q in last:
        finish(q, 1)
    sent(mix_full.at[pl.ds(0, nx * tok), :], p_send.at[0])
    for dx in range(1, nx):
        sent(mix_full.at[pl.ds(0, tok), :], p_send.at[1])
    w_drain(2)


def make_body(n_fs, n_tp, ny):
    nz, nx = n_fs // ny, n_tp // 2

    def body(
        mixed,
        residual,
        mix_weight,
        norm_gain,
        up_weight,
        gate_weight,
        conv_weight,
        conv_bias,
        down_weight,
    ):
        tok, width = residual.shape
        depth, (hid, wide) = mixed.shape[1], down_weight.shape
        piece = wide // 2 if wide % 256 == 0 else wide
        n_piece = width // piece
        dma = pltpu.SemaphoreType.DMA
        whole = pl.BlockSpec(memory_space=pl.ANY)
        small = pl.BlockSpec(memory_space=pltpu.VMEM)
        held = depth + 3 * hid + n_tp * tok + (3 * nx + 2) * tok
        lanes = (hid + 127) // 128 * 128
        held = held * width * 2 + n_tp * tok * lanes * 8 + (1 << 20)
        split = held <= VMEM
        return pl.pallas_call(
            functools.partial(layer_kernel, nz, ny, nx, split),
            out_shape=pltpu.VMEM((tok, width), bf16),
            in_specs=[whole] * 9,
            out_specs=small,
            scratch_shapes=[
                pltpu.VMEM((1, width), f32),
                pltpu.VMEM((3, hid), f32),
                pltpu.VMEM((hid,), f32),
                pltpu.VMEM((depth, width), bf16),
                pltpu.VMEM((hid, width), bf16),
                pltpu.VMEM((hid, width), bf16),
                pltpu.VMEM((hid, width), bf16),
                pltpu.VMEM((n_tp * tok, width), bf16),
                pltpu.VMEM((n_tp * tok + 16, hid), bf16),
                pltpu.VMEM((n_tp * tok, hid), bf16),
                pltpu.VMEM((n_tp * tok, hid) if split else (8, 128), f32),
                pltpu.VMEM((tok, depth), bf16),
                pltpu.VMEM((tok, width), bf16),
                pltpu.VMEM((nx, n_piece, tok, piece), bf16),
                pltpu.VMEM((nx, n_piece, tok, piece), bf16),
                pltpu.VMEM((max(nx - 1, 1), n_piece, tok, piece), bf16),
                dma((3,)),
                dma((2, n_fs, 2)),
                dma((3,)),
                dma((n_fs, max(nx - 1, 1))),
                dma((1,)),
                dma((2,)),
                dma((n_tp,)),
                dma((2,)),
                dma((n_piece, max(nx - 1, 1))),
                dma((n_piece // 2 + 1,)),
                dma((n_piece // 2 + 1, max(nx - 1, 1))),
                dma((9,)),
            ],
            compiler_params=pltpu.CompilerParams(
                collective_id=0, has_side_effects=True, vmem_limit_bytes=VMEM - 2 * tok * width * 2
            ),
        )(
            mixed,
            residual,
            mix_weight,
            up_weight.T,
            gate_weight.T,
            down_weight,
            norm_gain[None, :],
            conv_weight,
            conv_bias,
        )

    return body


def solution(mesh):
    coords = [getattr(d, "coords", None) for d in mesh.devices[:, 0]]
    n_fs, n_tp = mesh.shape["fs"], mesh.shape["tp"]
    ny = len({c[1] for c in coords}) if None not in coords else 1
    if n_fs % ny:
        ny = 1
    return jax.shard_map(
        make_body(n_fs, n_tp, ny),
        mesh=mesh,
        in_specs=(
            P(("fs", "tp"), None),
            P(("fs", "tp"), None),
            P(("fs", "tp"), None),
            P(),
            P("fs", "tp"),
            P("fs", "tp"),
            P(None, "tp"),
            P("tp"),
            P("tp", "fs"),
        ),
        out_specs=P(("fs", "tp"), None),
        check_vma=False,
    )
```
